128 devices in a mesh: sp: 16 (over z, x), tp: 8 (over y, core).
Axes of the slice: x: 4, y: 4, z: 4, core: 2. Of those that a mesh axis runs over, the one named last changes fastest.
Arguments:
- activation_sequence: bfloat16 [32768, 2, 2048], P(('sp', 'tp')), may hold values from -6 to 6
- rms_multiplier_vector: bfloat16 [2048], replicated, may hold values from 0.099609375 to 1.8984375
- linear_memory_source_matrix: bfloat16 [2048, 1024], P('sp', 'tp'), may hold values from -0.125 to 0.125
- linear_memory_exit_matrix: bfloat16 [2048, 1024], P('sp', 'tp'), may hold values from -0.125 to 0.125
- filter_exit_mask_matrix: bfloat16 [2048, 1024], P('sp', 'tp'), may hold values from -0.125 to 0.125
- filter_entry_mask_matrix: bfloat16 [2048, 1024], P('sp', 'tp'), may hold values from -0.125 to 0.125
- filter_source_matrix: bfloat16 [2048, 1024], P('sp', 'tp'), may hold values from -0.125 to 0.125
- memory_prefilter_taps: bfloat16 [4, 1024], P(None, 'tp'), may hold values from -3 to 3
- filter_taps_depthwise: bfloat16 [3, 1024], P(None, 'tp'), may hold values from -3.5 to 3.5
- fading_mask_diagonal_tiles: bfloat16 [2, 8, 128, 128], P(None, 'tp'), may hold values from -0.5 to 0.5
- entry_mask_diagonal_tiles: bfloat16 [2, 8, 128, 128], P(None, 'tp'), may hold values from -0.5 to 0.5
- fading_speed_per_channel: float32 [2, 1024], P(None, 'tp'), may hold values from 0 to 0.012
- speed_multiplier: float32 [32768], P('sp'), may hold values from 0.28 to 3.5
- jump_per_position: float32 [32768], P('sp'), may hold values from -2.1 to 0
- boundary_hidden_vectors: float32 [2, 2, 1024], P(None, None, 'tp'), may hold values from -6 to 6
- final_mixing_matrix: bfloat16 [2, 1024, 2048], P(None, None, ('sp', 'tp')), may hold values from -0.125 to 0.125
Outputs:
- mixed: bfloat16 [32768, 2, 2048], P(('sp', 'tp'))
The draws below stay inside these ranges and needn't reach their ends.
All inputs are finite; a program needn't handle non-finite values.
Results may differ from the reference program's by a relative error of at most 0.0084.
Values may be sent and summed in bfloat16 or wider, within the bound.
A program may use at most 192 MiB of HBM per device.

```python
import jax
import jax.numpy as jnp
from jax import lax

D = 2048
BR = 1024
BLK = 128
NB = 8
REC_TAPS = 4
CONV_TAPS = 3
BATCH = 2
TOK_SP = 2048
SEQ = 32768


def draw_fading_speed_per_channel(key, part):
    slow_key, pick_key, fast_key = jax.random.split(jax.random.fold_in(key, 11), 3)
    slow = jnp.exp(jax.random.uniform(slow_key, (2, BR), jnp.float32, jnp.log(0.005), jnp.log(0.04))) / SEQ
    fast = jnp.exp(jax.random.uniform(fast_key, (2, BR), jnp.float32, jnp.log(0.003), jnp.log(0.012)))
    chosen = jax.random.bernoulli(pick_key, 0.5, (2, BR))
    return jnp.where(chosen, slow, fast).astype(jnp.float32)


def draw_speed_multiplier(key, part):
    block_key, fine_key = jax.random.split(jax.random.fold_in(key, 23))
    count = SEQ // TOK_SP
    coarse = jnp.exp(jax.random.uniform(block_key, (count,), jnp.float32, jnp.log(0.4), jnp.log(2.5)))
    fine = jnp.exp(jax.random.uniform(fine_key, (SEQ,), jnp.float32, jnp.log(0.7), jnp.log(1.4)))
    return (jnp.repeat(coarse, TOK_SP) * fine).astype(jnp.float32)


def draw_jump_per_position(key, part):
    place_key, depth_key = jax.random.split(jax.random.fold_in(key, 37))
    places = jax.random.randint(place_key, (3,), 0, SEQ)
    depths = jax.random.uniform(depth_key, (3,), jnp.float32, jnp.log(0.5), jnp.log(0.8))
    hits = (jnp.arange(SEQ)[:, None] == places[None, :]).astype(jnp.float32)
    return jnp.dot(hits, depths).astype(jnp.float32)


def steps_of(own_key, extent, shards, smallest, top_value):
    loudness, own = 1.0, jax.random.fold_in(own_key, 6)
    for dim, blocks in shards:
        steps = jnp.exp(jax.random.uniform(jax.random.fold_in(own, dim), (blocks,), jnp.float32, smallest / len(shards), top_value / len(shards)))
        loudness = loudness * jnp.repeat(steps, extent[dim] // blocks).reshape([-1 if axis == dim else 1 for axis in range(len(extent))])
    return loudness


def gaussian(rng, shape, scale, most, pieces=(), kind=jnp.bfloat16):
    values = jax.random.normal(rng, shape, jnp.float32) * scale
    if len(pieces) > 0:
        values = steps_of(rng, shape, pieces, -0.22, 0.18) * values
    return jnp.clip(values, min=-most, max=most).astype(kind)


def setup_inputs(seed: int = 0) -> dict:
    arg_keys = jax.random.split(jax.random.key(seed), 17)
    activation_sequence = gaussian(arg_keys[0], (SEQ, BATCH, D), 1.0, 6.0, ((0, 128),))
    rms_multiplier_vector = jnp.clip(1.0 + 0.18 * jax.random.normal(arg_keys[1], (D,), jnp.float32), 0.099609375, 1.8984375).astype(jnp.bfloat16)
    linear_memory_source_matrix = gaussian(arg_keys[2], (D, BR), D ** -0.5, 0.125, ((0, 16), (1, 8)))
    linear_memory_exit_matrix = gaussian(arg_keys[3], (D, BR), D ** -0.5, 0.125, ((0, 16), (1, 8)))
    filter_exit_mask_matrix = gaussian(arg_keys[4], (D, BR), D ** -0.5, 0.125, ((0, 16), (1, 8)))
    filter_entry_mask_matrix = gaussian(arg_keys[5], (D, BR), D ** -0.5, 0.125, ((0, 16), (1, 8)))
    filter_source_matrix = gaussian(arg_keys[6], (D, BR), D ** -0.5, 0.125, ((0, 16), (1, 8)))
    memory_prefilter_taps = gaussian(arg_keys[7], (REC_TAPS, BR), REC_TAPS ** -0.5, 3.0, ((1, 8),))
    filter_taps_depthwise = gaussian(arg_keys[8], (CONV_TAPS, BR), CONV_TAPS ** -0.5, 3.5, ((1, 8),))
    fading_mask_diagonal_tiles = gaussian(arg_keys[9], (2, NB, BLK, BLK), BLK ** -0.5, 0.5, ((1, 8),))
    entry_mask_diagonal_tiles = gaussian(arg_keys[10], (2, NB, BLK, BLK), BLK ** -0.5, 0.5, ((1, 8),))
    fading_speed_per_channel = draw_fading_speed_per_channel(jax.random.fold_in(arg_keys[16], 71), 0)
    speed_multiplier = draw_speed_multiplier(jax.random.fold_in(arg_keys[16], 71), 0)
    jump_per_position = draw_jump_per_position(jax.random.fold_in(arg_keys[16], 71), 0)
    boundary_hidden_vectors = gaussian(arg_keys[14], (2, BATCH, BR), 1.0, 6.0, ((2, 8),), jnp.float32)
    final_mixing_matrix = gaussian(arg_keys[15], (2, BR, D), (2 * BR) ** -0.5, 0.125, ((2, 128),))
    return {"activation_sequence": activation_sequence, "rms_multiplier_vector": rms_multiplier_vector, "linear_memory_source_matrix": linear_memory_source_matrix, "linear_memory_exit_matrix": linear_memory_exit_matrix, "filter_exit_mask_matrix": filter_exit_mask_matrix, "filter_entry_mask_matrix": filter_entry_mask_matrix, "filter_source_matrix": filter_source_matrix, "memory_prefilter_taps": memory_prefilter_taps, "filter_taps_depthwise": filter_taps_depthwise, "fading_mask_diagonal_tiles": fading_mask_diagonal_tiles, "entry_mask_diagonal_tiles": entry_mask_diagonal_tiles, "fading_speed_per_channel": fading_speed_per_channel, "speed_multiplier": speed_multiplier, "jump_per_position": jump_per_position, "boundary_hidden_vectors": boundary_hidden_vectors, "final_mixing_matrix": final_mixing_matrix}


epsilon = 1e-06
decay_factor_scale = 8.0

def combine(earlier, later):
    return (earlier[0] * later[0], later[0] * earlier[1] + later[1])

def reference(activation_sequence, rms_multiplier_vector, linear_memory_source_matrix, linear_memory_exit_matrix, filter_exit_mask_matrix, filter_entry_mask_matrix, filter_source_matrix, memory_prefilter_taps, filter_taps_depthwise, fading_mask_diagonal_tiles, entry_mask_diagonal_tiles, fading_speed_per_channel, speed_multiplier, jump_per_position, boundary_hidden_vectors, final_mixing_matrix):
    widened = activation_sequence.astype(jnp.float32)
    normed = (widened * lax.rsqrt(lax.optimization_barrier(jnp.mean(widened * widened, axis=-1, keepdims=True)) + epsilon) * rms_multiplier_vector.astype(jnp.float32)).astype(jnp.bfloat16)
    flat_rows = normed.reshape(SEQ * BATCH, D)

    def project(weight):
        return jnp.dot(flat_rows, weight, preferred_element_type=jnp.float32).astype(jnp.bfloat16).reshape(SEQ, BATCH, BR)
    rec_in = project(linear_memory_source_matrix)
    rec_gate = project(linear_memory_exit_matrix)
    conv_out = project(filter_exit_mask_matrix)
    conv_gate = project(filter_entry_mask_matrix)
    conv_in = project(filter_source_matrix)
    shaken = (conv_gate.astype(jnp.float32) * conv_in.astype(jnp.float32)).astype(jnp.bfloat16)
    padded = jnp.pad(rec_in, ((2, 1), (0, 0), (0, 0))).astype(jnp.float32)
    rec_conv = jnp.zeros((SEQ, BATCH, BR), jnp.float32)
    for offset in range(REC_TAPS):
        rec_conv = rec_conv + memory_prefilter_taps[offset].astype(jnp.float32) * padded[offset:offset + SEQ]
    rec_conv = rec_conv.astype(jnp.bfloat16)
    padded_s = jnp.pad(shaken, ((1, 1), (0, 0), (0, 0))).astype(jnp.float32)
    short = jnp.zeros((SEQ, BATCH, BR), jnp.float32)
    for offset in range(CONV_TAPS):
        short = short + filter_taps_depthwise[offset].astype(jnp.float32) * padded_s[offset:offset + SEQ]
    conv_y = (conv_out.astype(jnp.float32) * short).astype(jnp.bfloat16)
    blocks = rec_conv.astype(jnp.float32).reshape(SEQ, BATCH, NB, BLK)
    widened_conv = rec_conv.astype(jnp.float32)
    tempo_column = speed_multiplier.astype(jnp.float32)[:, None, None]
    jump_vertical_vector = jump_per_position.astype(jnp.float32)[:, None, None]
    states = jnp.zeros((SEQ, BATCH, BR), jnp.float32)
    for scan_direction in range(2):
        recurrence_preactivation = jnp.einsum('lbnd,nde->lbne', blocks, fading_mask_diagonal_tiles[scan_direction].astype(jnp.float32)).reshape(SEQ, BATCH, BR)
        pre_i = jnp.einsum('lbnd,nde->lbne', blocks, entry_mask_diagonal_tiles[scan_direction].astype(jnp.float32)).reshape(SEQ, BATCH, BR)
        log_decay = -decay_factor_scale * jax.nn.sigmoid(recurrence_preactivation) * fading_speed_per_channel[scan_direction] * tempo_column + jump_vertical_vector
        decay = jnp.exp(log_decay)
        drive = jnp.sqrt(-jnp.expm1(2.0 * log_decay)) * jax.nn.sigmoid(pre_i) * widened_conv
        acum, bcum = lax.associative_scan(combine, (decay, drive), axis=0, reverse=scan_direction == 1)
        states = states + bcum + acum * boundary_hidden_vectors[scan_direction][None]
    rec_out = (states * jax.nn.gelu(rec_gate.astype(jnp.float32))).astype(jnp.bfloat16)
    total = jnp.dot(rec_out.reshape(SEQ * BATCH, BR), final_mixing_matrix[0], preferred_element_type=jnp.float32)
    total = total + jnp.dot(conv_y.reshape(SEQ * BATCH, BR), final_mixing_matrix[1], preferred_element_type=jnp.float32)
    return total.astype(jnp.bfloat16).reshape(SEQ, BATCH, D)
```

```python
import jax
import jax.numpy as jnp
from jax import lax
from jax.experimental import pallas as pl
from jax.experimental.pallas import tpu as pltpu
from jax.sharding import PartitionSpec as P

MESH = pl.DeviceIdType.MESH
f32, bf16 = jnp.float32, jnp.bfloat16

EPS = 1e-06
RING = 4
OWN = 512
STEPS = 64
WIDE = 2048
LANES = 128
POOL = 32

SRC, GATES, CGATE, CIN, COUT, EXIT, W_END = 0, 128, 160, 288, 416, 544, 672
OUT_ROWS = 256

PIECES = (
    ("w", ((0, 64), (64, 112), (112, 160))),
    ("w", ((160, 240), (240, 320), (320, 416))),
    ("w", ((416, 496), (496, 592), (592, 672))),
    ("o", ((0, 80), (80, 160), (160, 256))),
)
ORDERS = (("y", "x", "z"), ("x", "z", "y"), ("z", "y", "x"))
NEAR = (0, -1, 1, 2)
FORWARD = {1: (0, -1), -1: (1, 2)}


def turn_of(piece):
    return 1 if piece % 2 == 0 else -1


def group_of(m):
    piece, colour, phase, kind, way, r = m
    if kind == "pass":
        return (piece, colour, 3, r, 1)
    if phase == 0:
        return (piece, colour, 0, 2 if kind == "fwd" else (0 if way == 1 else 1), 1)
    first = 3 + 7 * (phase - 1)
    if kind == "fwd":
        return (piece, colour, phase, first + 6, 4)
    alone = FORWARD[way]
    place = alone.index(r) if r in alone else 2
    return (piece, colour, phase, first + place + (0 if way == 1 else 3), 1 if r in alone else 2)


def messages(piece, colour):
    found = {}
    up = turn_of(piece)

    def own(phase, way, r):
        return (piece, colour, phase, "own", way, r)

    def fwd(phase, way, r):
        return (piece, colour, phase, "fwd", way, r)

    def here(*given):
        return tuple(dict.fromkeys(group_of(m) for m in given))

    ready = {-1: here(own(0, 1, 0)), 1: here(own(0, -1, 0)), 2: here(fwd(0, up, 0)), 0: ()}
    first = here(own(0, 1, 0), own(0, -1, 0), fwd(0, up, 0))
    for way in (1, -1):
        found[own(0, way, 0)] = ()
    found[fwd(0, up, 0)] = here(own(0, up, 0))
    for phase in (1, 2):
        for r in NEAR:
            for way in (1, -1):
                found[own(phase, way, r)] = ready[r]
        for way in (1, -1):
            for r in FORWARD[way]:
                found[fwd(phase, way, r)] = here(own(phase, way, r))
        ready = {
            0: first,
            -1: here(*(own(phase, 1, r) for r in NEAR)),
            1: here(*(own(phase, -1, r) for r in NEAR)),
            2: here(fwd(phase, 1, 0)),
        }
    if piece == 3:
        before = here(*(m for m in found if m[2] < 2))
        for slot, r in enumerate((0, -1, 1, 2)):
            found[(piece, colour, 3, "pass", 0, slot)] = before if r == 0 else ready[r]
    return found


def size(m):
    first, last = PIECES[m[0]][1][m[1]]
    return (last - first) * 0.25 * (1, 1, 4, 16)[m[2]]


RATE, HOP = 44.0, 2.2
SIDE_RATE, SIDE_HOP = 450.0, 1.4

STAGES = (
    ("norm_own", 4, 1.5, ()),
    ("norm_other", 4, 1.5, ("rows",)),
    ("norm_edges", 1, 0.3, ("edges",)),
    ("source", 4, 0.8, ("norm_own", "norm_other", "norm_edges", 0)),
    ("source_edges", 1, 0.6, ("source",)),
    ("gates", 4, 1.95, ("source_edges", "small")),
    ("totals", 1, 1.3, ("gates",)),
    ("hear0", 1, 0.4, ("told0",)),
    ("hear1", 1, 0.4, ("told1",)),
    ("hear2", 1, 0.5, ("told2",)),
    ("shake", 4, 1.4, ("norm_own", "norm_other", "norm_edges", 1)),
    ("shake_edges", 1, 0.8, ("shake",)),
    ("exit_gate", 4, 0.78, (2, "norm_other")),
    ("conv", 4, 0.75, (2, "shake_edges")),
    ("states", 1, 1.5, ("hear2", "exit_gate")),
    ("result", 8, 0.85, (3, "swapped0", "swapped1")),
)
BACKLOG = 1.0


def PRIORITY(m):
    return (m[0], m[2])


def plan():
    deps = {}
    for piece in range(4):
        for colour in range(3):
            deps.update(messages(piece, colour))
    groups = {}
    for m in deps:
        groups.setdefault(group_of(m), []).append(m)
    clock, link, coming, arrive, sent, got = 0.0, {}, {}, {}, set(), set()
    times = {"rows": 6.0, "edges": 4.0, "small": 6.0}
    order, done, progress = [], set(), {}

    def send_ready():
        ready = [m for m in deps if m not in sent and all(d in got for d in deps[m])]
        for m in sorted(ready, key=PRIORITY):
            side = m[3] == "pass"
            wire = "side" if side else (ORDERS[m[1]][m[2]], m[4])
            if link.get(wire, 0.0) - clock > BACKLOG:
                continue
            link[wire] = max(clock, link.get(wire, 0.0)) + size(m) / (SIDE_RATE if side else RATE)
            arrive[m] = link[wire] + (SIDE_HOP if side else HOP)
            sent.add(m)
            order.append(("send", m))
            g = group_of(m)
            if all(n in sent for n in groups[g]):
                coming[g] = max(arrive[n] for n in groups[g])

    def met(need):
        if isinstance(need, int):
            return all(g in got for g in groups if g[0] == need)
        return need in done or times.get(need, 1e9) <= clock

    current = None
    send_ready()
    while len(done) < len(STAGES):
        here = sorted((m for m in coming if m not in got and coming[m] <= clock), key=lambda m: (m[0], coming[m]))
        if here:
            m = here[0]
            got.add(m)
            order.append(("wait", m))
            clock += 0.03
            send_ready()
            continue
        send_ready()
        if current is None:
            for n, stage in enumerate(STAGES):
                if stage[0] not in done and all(met(need) for need in stage[3]):
                    current = stage
                    break
        quick = next(
            (st for st in STAGES if st[0].startswith("hear") and st[0] not in done and all(met(k) for k in st[3])), None
        )
        if quick is not None:
            order.append(("unit", quick[0], 0))
            clock += quick[2]
            done.add(quick[0])
            level = int(quick[0][4])
            if level < 2:
                times[f"told{level + 1}"] = clock + 3.5
            if current is quick:
                current = None
            continue
        if current is not None:
            name, units, cost, _ = current
            i = progress.get(name, 0)
            order.append(("unit", name, i))
            clock += cost
            progress[name] = i + 1
            if i + 1 == units:
                done.add(name)
                current = None
                if name == "totals":
                    times["told0"] = clock + 3.5
                if name == "conv":
                    times["swapped1"] = clock + 3.0
                if name == "states":
                    times["swapped0"] = clock + 3.0
            continue
        if any(m not in sent and all(d in got for d in deps[m]) for m in deps):
            clock += 0.25
            continue
        later = [t for m, t in coming.items() if m not in got] + [t for t in times.values() if t > clock]
        clock = min(t for t in later if t > clock)
    return order, clock


def wrap(i):
    return lax.rem(i + RING, RING)


def rows_of(shape):
    return lax.broadcasted_iota(jnp.int32, shape, 0)


def turn(v, by):
    return pltpu.roll(v, by, 0)


def spread(v, first):
    row = rows_of(v.shape)
    v = jnp.where((row >= first) & (row < first + 2), v, 0.0)
    v = v + turn(v, 2)
    return v + turn(v, 4)


def kernel(
    x_in, gain_in, src_in, exit_in, cout_in, cgate_in, cin_in, taps_in, ctaps_in, fade_in, entry_in, speed_in,
    tempo_in, jump_in, edge_in, out_w, out,
    XR, XE, X, G, Wo, GN, TB, CB, SB, BB, PM, SM, MJ, Rp, Sp, Hh, A, U, GL, ACT, ACTS, SEG, PRE, XS,
    lsem, wsem, pool, grecv, frecv, xrecv, hrecv, srecv, erecv, arecv,
):
    sp, tp = lax.axis_index("sp"), lax.axis_index("tp")
    me = {"z": sp // 4, "x": lax.rem(sp, 4), "y": tp // 2}
    c = lax.rem(tp, 2)
    z, x, y = me["z"], me["x"], me["y"]
    q = sp * 4 + y

    def device(at, core):
        return {"sp": at["z"] * 4 + at["x"], "tp": at["y"] * 2 + core}

    def along(d, by):
        return {**me, d: wrap(me[d] + by)}

    sibling = device(me, 1 - c)
    ahead = lax.rem(q + 1, 64)
    behind = lax.rem(q + 63, 64)

    def chip(number, core):
        return {"sp": number // 4, "tp": lax.rem(number, 4) * 2 + core}

    barrier = pltpu.get_barrier_semaphore()

    def hello(to):
        pl.semaphore_signal(barrier, inc=1, device_id=to, device_id_type=MESH)

    hello(sibling)
    for d in ("z", "x", "y"):
        for by in (1, 2, 3):
            hello(device(along(d, by), c))
    hello(chip(behind, 1))
    hello(chip(ahead, 0))

    def own_rows(first, count):
        return G.at[z, x, y, pl.ds(first, count)]

    sp16 = pl.ds(pl.multiple_of(sp * 16, 16), 16)
    pairs = [
        (src_in, own_rows(SRC, 128)),
        (fade_in.at[sp16], own_rows(GATES, 16)),
        (entry_in.at[sp16], own_rows(GATES + 16, 16)),
        (cgate_in, own_rows(CGATE, 128)),
        (cin_in, own_rows(CIN, 128)),
        (cout_in, own_rows(COUT, 128)),
        (exit_in, own_rows(EXIT, 128)),
        (gain_in, GN),
        (taps_in, TB),
        (ctaps_in, CB),
        (speed_in, SB),
        (edge_in, BB),
        (tempo_in, PM.at[0]),
        (jump_in, PM.at[1]),
    ]
    pairs += [(x_in.at[pl.ds(seg * STEPS, STEPS)], XR.at[c, :, seg]) for seg in range(4)]
    local = [pltpu.make_async_copy(a, b, lsem.at[n]) for n, (a, b) in enumerate(pairs)]
    out_local = [
        pltpu.make_async_copy(
            out_w.at[n // 8, :, pl.ds((n % 8) * LANES, LANES)], Wo.at[z, x, y, c, pl.ds(n * 16, 16)], wsem.at[n]
        )
        for n in range(16)
    ]
    for copy in local + out_local:
        copy.start()
    pl.semaphore_wait(barrier, 12)

    def remote(src, dst, send, recv, to):
        return pltpu.make_async_remote_copy(
            src_ref=src, dst_ref=dst, send_sem=pool.at[0] if send is None else send, recv_sem=recv, device_id=to, device_id_type=MESH
        )

    sends = []

    def go(make, *given):
        n = len(sends)
        if n >= POOL:
            finish(n - POOL)
        make(*given, send=pool.at[n % POOL]).start()
        sends.append((make, given))

    def finish(n):
        make, given = sends[n]
        make(*given, send=pool.at[n % POOL]).wait_send()

    def rows_copy(seg, send=None):
        return remote(
            x_in.at[pl.ds(seg * STEPS, STEPS)], XR.at[c, :, seg], send, xrecv.at[seg], sibling
        )

    target = jnp.where(c == 1, ahead, behind)

    def edge_copy(core, slot, send=None):
        return remote(
            x_in.at[pl.ds(c * 254, 2)], XE.at[pl.ds((1 - c) * 2, 2)], send, hrecv.at[slot], chip(target, core)
        )

    for seg in range(4):
        go(rows_copy, seg)
    for core in range(2):
        go(edge_copy, core, 1 - c)

    def region(piece, colour, phase, i, r, count=1):
        kind, parts = PIECES[piece]
        first, last = parts[colour]
        a, b, d = ORDERS[colour]
        where = dict(me)
        if phase == 0:
            where[a] = i
        elif phase == 1:
            where[a], where[b] = wrap(me[a] + r), i
        else:
            where[a], where[b], where[d] = slice(None), wrap(me[b] + r), i
            if phase == 3:
                where[b] = slice(None)
        if count > 1:
            where[(a, b)[phase - 1]] = pl.ds(0, count)
        rows = pl.ds(first, last - first)
        if kind == "w":
            return G.at[where["z"], where["x"], where["y"], rows]
        return Wo.at[where["z"], where["x"], where["y"], c, rows]

    def message(m, send=None):
        piece, colour, phase, kind, way, r = m
        if kind == "pass":
            d = ORDERS[colour][2]
            ref = region(piece, colour, 3, wrap(me[d] + (0, -1, 1, 2)[r]), 0)
            return remote(ref, ref, send, frecv.at[colour, r], sibling)
        d = ORDERS[colour][phase]
        block = me[d] if kind == "own" else wrap(me[d] - way)
        ref = region(piece, colour, phase, block, r)
        return remote(ref, ref, send, grecv.at[(piece * 3 + colour) * 17 + group_of(m)[3]], device(along(d, way), c))

    def group_here(g):
        piece, colour, phase, place, count = g
        ref = region(piece, colour, phase, 0, 0, count)
        remote(ref, ref, None, grecv.at[(piece * 3 + colour) * 17 + place], sibling).wait_recv()

    for copy in local[7:14]:
        copy.wait()
    for row in range(4):
        SM[y, row : row + 1, :] = TB[row : row + 1, :].astype(f32)
    for row in range(3):
        SM[y, 4 + row : 5 + row, :] = CB[row : row + 1, :].astype(f32)
    for row in range(2):
        SM[y, 7 + row : 8 + row, :] = SB[row : row + 1, :]
        for b in range(2):
            SM[y, 9 + 2 * row + b : 10 + 2 * row + b, :] = BB[row, b : b + 1, :]
    SM[y, 13:16, :] = jnp.zeros((3, LANES), f32)

    def small_copy(by, send=None):
        return remote(SM.at[y], SM.at[y], send, srecv.at[by - 1], device(along("y", by), c))

    def positions():
        seg = rows_of((8, LANES)) // 2
        for n in range(2):
            for rc in range(2):
                lines = [
                    jnp.broadcast_to(PM[n, pl.ds(4 * y + rc * 2 + k, 1), :], (8, LANES)) for k in range(2)
                ]
                v = jnp.where(
                    seg == 0,
                    lines[0],
                    jnp.where(
                        seg == 1, pltpu.roll(lines[0], 64, 1), jnp.where(seg == 2, lines[1], pltpu.roll(lines[1], 64, 1))
                    ),
                )
                for j in range(STEPS):
                    MJ[n, rc * OWN + j * 8 : rc * OWN + j * 8 + 8, :] = jnp.broadcast_to(v[:, j : j + 1], (8, LANES))

    def scaled(parts, alive=None):
        total = parts[0] * parts[0]
        for v in parts[1:]:
            total = total + v * v
        r = lax.rsqrt(jnp.sum(total, axis=1, keepdims=True) * (1.0 / WIDE) + EPS)
        if alive is not None:
            r = r * alive
        r = jnp.broadcast_to(r, parts[0].shape)
        return [(v * r) * GN[n : n + 1, :].astype(f32) for n, v in enumerate(parts)]

    def norm_unit(rc, i):
        def one(k, _):
            j = i * 16 + k * 2
            parts = [
                XR[rc, pl.ds(j, 2), :, :, n * LANES : (n + 1) * LANES].astype(f32).reshape(16, LANES) for n in range(16)
            ]
            rows = pl.ds(pl.multiple_of(rc * OWN + j * 8, 16), 16)
            for n, v in enumerate(scaled(parts)):
                X[rows, n * LANES : (n + 1) * LANES] = v.astype(bf16)
            return 0

        lax.fori_loop(0, 8, one, 0)

    def norm_edges():
        row = rows_of((8, 1))
        alive = jnp.where(row < 4, jnp.where(q > 0, 1.0, 0.0), jnp.where(q < 63, 1.0, 0.0))
        parts = [XE[:, :, n * LANES : (n + 1) * LANES].astype(f32).reshape(8, LANES) for n in range(16)]
        for n, v in enumerate(scaled(parts, alive)):
            lane = slice(n * LANES, (n + 1) * LANES)
            X[2 * OWN : 2 * OWN + 16, lane] = jnp.concatenate([turn(v, 6), turn(v, 4)], axis=0).astype(bf16)
            X[2 * OWN + 16 : 2 * OWN + 32, lane] = jnp.concatenate([turn(v, 4), turn(v, 4)], axis=0).astype(bf16)

    def weight(row, yp):
        parts = [G[:, :, 2 * yp + h, pl.ds(row, LANES), :].reshape(WIDE, LANES) for h in range(2)]
        return jnp.concatenate(parts, axis=1)

    def project(rows, w):
        return jnp.dot(X[rows, :], w, preferred_element_type=f32)

    def block(work, i):
        yp, rc = i // 2, lax.rem(i, 2)
        work(yp, rc, pl.ds(pl.multiple_of(rc * OWN, OWN), OWN))

    main = pl.ds(16, OWN)
    edges = pl.ds(2 * OWN, 32)

    def pads(Rp):
        for yp in range(2):
            row = rows_of((8, 256))
            for rc in range(2):
                for j in range(2):
                    own = Rp[yp, rc, pl.ds(16 + (STEPS - 2 + j) * 8, 8), :]
                    prior = Hh[yp, pl.ds(8 * j, 8), :] if rc == 0 else Rp[yp, 0, pl.ds(16 + (STEPS - 2 + j) * 8, 8), :]
                    Rp[yp, rc, pl.ds(8 * j, 8), :] = jnp.where(row < 2, turn(prior, 2), turn(own, 2))
                own = Rp[yp, rc, pl.ds(16, 8), :]
                later = Rp[yp, 1, pl.ds(16, 8), :] if rc == 0 else Hh[yp, pl.ds(16, 8), :]
                Rp[yp, rc, pl.ds(16 + OWN, 8), :] = jnp.where(row >= 6, turn(later, 6), turn(own, 6))

    def source(i):
        def work(yp, rc, rows):
            Rp[yp, rc, main, :] = project(rows, weight(SRC, yp))

        block(work, i)

    def source_edges():
        for yp in range(2):
            Hh[yp] = project(edges, weight(SRC, yp))
        pads(Rp)

    def taps(yp, row):
        return jnp.concatenate([SM[2 * yp + h, pl.ds(row, 1), :] for h in range(2)], axis=1)

    GB = 128

    def gates(i):
        def one(k, _):
            gate_rows(i // 2, lax.rem(i, 2), k)
            return 0

        lax.fori_loop(0, 4, one, 0)

    def gate_rows(yp, rc, blk):
        base = pl.multiple_of(blk * GB, GB)
        rc_rows = jnp.zeros((GB, 256), f32)
        for k in range(4):
            rc_rows = rc_rows + taps(yp, k) * Rp[yp, rc, pl.ds(base + 8 * k, GB), :]
        narrow = rc_rows.astype(bf16)
        wide = narrow.astype(f32)
        at = pl.ds(pl.multiple_of(rc * OWN + blk * GB, GB), GB)
        tempo, jump = MJ[0, at, :], MJ[1, at, :]
        for h in range(2):
            lane = slice(h * LANES, (h + 1) * LANES)
            yy = 2 * yp + h
            maps = [
                    G[pl.ds(2 * d, 2), :, yy, pl.ds(GATES + 16 * kind, 16), :].reshape(LANES, LANES)
                    for kind in range(2)
                    for d in range(2)
                ]
            for d in range(2):
                pre = jnp.dot(
                    narrow[:, lane], jnp.concatenate([maps[d], maps[2 + d]], axis=1), preferred_element_type=f32
                )
                speed = SM[yy, pl.ds(7 + d, 1), :] * -4.0
                la = (1.0 + jnp.tanh(0.5 * pre[:, :LANES])) * (speed * tempo) + jump
                decay = jnp.exp(la)
                t = 2.0 * la
                near = -t * (1.0 + t * (0.5 + t * (1.0 / 6.0 + t * (1.0 / 24.0 + t * (1.0 / 120.0)))))
                rest = jnp.where(t > -0.1, near, 1.0 - decay * decay)
                opening = 0.5 + 0.5 * jnp.tanh(0.5 * pre[:, LANES:])
                A[d, yp, rc, pl.ds(base, GB), lane] = decay
                U[d, yp, rc, pl.ds(base, GB), lane] = jnp.sqrt(rest) * opening * wide[:, lane]

    PAIRS = [(yp, rc) for yp in range(2) for rc in range(2)]

    def tile(ref, d, yp, rc, j):
        return ref[d, yp, rc, pl.ds(pl.multiple_of(j * 8, 8), 8), :]

    def totals():
        def one(i, state):
            new = []
            for d in range(2):
                j = i if d == 0 else STEPS - 1 - i
                for n, (yp, rc) in enumerate(PAIRS):
                    sa, sb = state[d * 4 + n]
                    a = tile(A, d, yp, rc, j)
                    new.append((sa * a, sb * a + tile(U, d, yp, rc, j)))
            return tuple(new)

        start = tuple((jnp.ones((8, 256), f32), jnp.zeros((8, 256), f32)) for _ in range(8))
        end = lax.fori_loop(0, STEPS, one, start)
        row = rows_of((8, 256))
        for yp in range(2):
            whole = []
            for d in range(2):
                ends = []
                for rc in range(2):
                    a, b = end[d * 4 + yp * 2 + rc]
                    for by in (2, 4):
                        shift = by if d == 0 else 8 - by
                        inside = (row >= by) if d == 0 else (row < 8 - by)
                        pa, pb = turn(a, shift), turn(b, shift)
                        b = jnp.where(inside, a * pb + b, b)
                        a = jnp.where(inside, a * pa, a)
                    SEG[d, yp, rc, 0], SEG[d, yp, rc, 1] = a, b
                    ends.append((spread(a, 6 if d == 0 else 0), spread(b, 6 if d == 0 else 0)))
                first, second = ends if d == 0 else ends[::-1]
                whole.append((first[0] * second[0], second[0] * first[1] + second[1]))
            put(0, y, yp, whole)

    def put(level, slot, yp, whole):
        row = rows_of((8, 256))
        (fa, fb), (ba, bb) = whole
        XS[level, slot, :, yp * 256 : (yp + 1) * 256] = jnp.where(
            row < 2, fa, jnp.where(row < 4, fb, jnp.where(row < 6, ba, bb))
        )

    AXES = ("y", "x", "z")

    def share(level, by, send=None):
        d = AXES[level]
        ref = XS.at[level, me[d]]
        k = level * 3 + by - 1
        return remote(ref, ref, send, erecv.at[k], device(along(d, by), c))

    def tell(level):
        for by in (1, 2, 3):
            go(share, level, by)

    def combine(early, late):
        return early[0] * late[0], late[0] * early[1] + late[1]

    def hear(level):
        for by in (1, 2, 3):
            share(level, by).wait_recv()
        m = me[AXES[level]]
        for yp in range(2):
            one = (jnp.ones((8, 256), f32), jnp.zeros((8, 256), f32))
            whole = []
            for d in range(2):
                total, prefix = one, one
                for i in range(4) if d == 0 else range(3, -1, -1):
                    v = XS[level, i, :, yp * 256 : (yp + 1) * 256]
                    item = (spread(v, 4 * d), spread(v, 4 * d + 2))
                    passed = (i < m) if d == 0 else (i > m)
                    longer = combine(prefix, item)
                    prefix = tuple(jnp.where(passed, n, o) for n, o in zip(longer, prefix))
                    total = combine(total, item)
                whole.append(total)
                PRE[level, yp, d, 0], PRE[level, yp, d, 1] = prefix
            if level < 2:
                put(level + 1, me[AXES[level + 1]], yp, whole)
        if level < 2:
            tell(level + 1)

    def entering():
        row = rows_of((8, 256))
        even = (row % 2) == 0
        for yp in range(2):
            for d in range(2):
                h = jnp.where(even, taps(yp, 9 + 2 * d), taps(yp, 10 + 2 * d))
                for level in (2, 1, 0):
                    a, b = PRE[level, yp, d, 0], PRE[level, yp, d, 1]
                    h = a * h + b
                for rc in (0, 1) if d == 0 else (1, 0):
                    a, b = SEG[d, yp, rc, 0], SEG[d, yp, rc, 1]
                    shift = 2 if d == 0 else 6
                    inside = (row >= 2) if d == 0 else (row < 6)
                    pa = jnp.where(inside, turn(a, shift), 1.0)
                    pb = jnp.where(inside, turn(b, shift), 0.0)
                    SEG[d, yp, rc, 0] = pa * h + pb
                    last = 6 if d == 0 else 0
                    h = spread(a, last) * h + spread(b, last)

    def exit_gate(i):
        def work(yp, rc, rows):
            v = project(rows, weight(EXIT, yp))
            inner = v * (0.7978845608028654 + 0.035677408136300125 * v * v)
            GL[yp, rc] = 0.5 * v * (1.0 + jnp.tanh(inner))

        block(work, i)

    def states():
        def forth(i, state):
            new = []
            for n, (yp, rc) in enumerate(PAIRS):
                h = tile(A, 0, yp, rc, i) * state[n] + tile(U, 0, yp, rc, i)
                U[0, yp, rc, pl.ds(pl.multiple_of(i * 8, 8), 8), :] = h
                new.append(h)
            return tuple(new)

        def back(i, state):
            new = []
            low = STEPS - 2 - 2 * i
            rows16 = pl.ds(pl.multiple_of(low * 8, 16), 16)
            for n, (yp, rc) in enumerate(PAIRS):
                h1 = tile(A, 1, yp, rc, low + 1) * state[n] + tile(U, 1, yp, rc, low + 1)
                h0 = tile(A, 1, yp, rc, low) * h1 + tile(U, 1, yp, rc, low)
                both = jnp.concatenate([h0, h1], axis=0) + U[0, yp, rc, rows16, :]
                done = (both * GL[yp, rc, rows16, :]).astype(bf16)
                for h in range(2):
                    ACT[rc, 0, 2 * yp + h, rows16, :] = done[:, h * LANES : (h + 1) * LANES]
                new.append(h0)
            return tuple(new)

        lax.fori_loop(0, STEPS, forth, tuple(SEG[0, yp, rc, 0] for yp, rc in PAIRS))
        lax.fori_loop(0, STEPS // 2, back, tuple(SEG[1, yp, rc, 0] for yp, rc in PAIRS))

    def shake(i):
        def work(yp, rc, rows):
            Sp[yp, rc, main, :] = project(rows, weight(CGATE, yp)) * project(rows, weight(CIN, yp))

        block(work, i)

    def shake_edges():
        for yp in range(2):
            Hh[yp] = project(edges, weight(CGATE, yp)) * project(edges, weight(CIN, yp))
        pads(Sp)

    def conv(i):
        def work(yp, rc, rows):
            v = project(rows, weight(COUT, yp))
            s = jnp.zeros((OWN, 256), f32)
            for k in range(3):
                s = s + taps(yp, 4 + k) * Sp[yp, rc, pl.ds(8 + 8 * k, OWN), :]
            done = (v * s).astype(bf16)
            for h in range(2):
                ACT[rc, 1, 2 * yp + h] = done[:, h * LANES : (h + 1) * LANES]

        block(work, i)

    def swap(m, send=None):
        return remote(ACT.at[1 - c, m], ACTS.at[m], send, arecv.at[m], sibling)

    def result(i):
        zz, xx = i // 2, lax.rem(i, 2) * 2
        left, right = [], []
        for own in range(2):
            core = c if own == 0 else 1 - c
            for m in range(2):
                for yy in range(4):
                    left.append(ACT[c, m, yy] if own == 0 else ACTS[m, yy])
                    k16 = pl.ds(pl.multiple_of((m * 8 + 2 * yy + core) * 16, 16), 16)
                    right.append(Wo[zz, pl.ds(xx, 2), :, :, k16, :].reshape(256, LANES))
        v = lax.dot_general(
            jnp.concatenate(left, axis=1), jnp.concatenate(right, axis=1),
            (((1,), (1,)), ((), ())), preferred_element_type=f32,
        )
        v = v.astype(bf16).reshape(STEPS, 4, 2, 256)
        for seg in range(4):
            out[seg * STEPS : (seg + 1) * STEPS, :, pl.ds(pl.multiple_of(i * 256, 256), 256)] = v[:, seg]

    def before_other():
        for seg in range(4):
            rows_copy(seg).wait_recv()

    def before_edges():
        for slot in range(2):
            edge_copy(0, slot).wait_recv()

    def before_gates():
        for by in (1, 2, 3):
            small_copy(by).wait_recv()
        positions()

    def before_result():
        for m in (1, 0):
            with jax.named_scope(f"swap_{m}"):
                swap(m).wait_recv()
        for colour in range(3):
            for r in range(4):
                with jax.named_scope(f"pass_{colour}_{r}"):
                    message((3, colour, 3, "pass", 0, r)).wait_recv()

    def after_own():
        for by in (1, 2, 3):
            go(small_copy, by)

    def last_states():
        entering()
        states()

    def await_local():
        for copy in local[14:]:
            copy.wait()

    stages = {
        "norm_own": (await_local, lambda i: norm_unit(c, i), after_own),
        "norm_other": (before_other, lambda i: norm_unit(1 - c, i), None),
        "norm_edges": (before_edges, lambda i: norm_edges(), None),
        "source": (None, source, None),
        "source_edges": (None, lambda i: source_edges(), None),
        "gates": (before_gates, gates, None),
        "totals": (None, lambda i: totals(), lambda: tell(0)),
        "hear0": (None, lambda i: hear(0), None),
        "hear1": (None, lambda i: hear(1), None),
        "hear2": (None, lambda i: hear(2), None),
        "shake": (None, shake, None),
        "shake_edges": (None, lambda i: shake_edges(), None),
        "exit_gate": (None, exit_gate, None),
        "conv": (None, conv, lambda: go(swap, 1)),
        "states": (None, lambda i: last_states(), lambda: go(swap, 0)),
        "result": (before_result, result, None),
    }
    held = {0: local[0:3], 1: local[3:5], 2: local[5:7], 3: out_local}
    units = {name: count for name, count, _, _ in STAGES}

    def follow(step):
        if step[0] == "send":
            for copy in held.pop(step[1][0], ()):
                copy.wait()
            go(message, step[1])
        elif step[0] == "wait":
            if step[1][2] < 3:
                group_here(step[1])
        else:
            stages[step[1]][1](0)

    order, _ = plan()
    n = 0
    while n < len(order):
        step = order[n]
        if step[0] != "unit" or units[step[1]] == 1:
            if step[0] == "unit":
                before, work, after = stages[step[1]]
                with jax.named_scope(step[1]):
                    if before is not None:
                        before()
                    work(0)
                    if after is not None:
                        after()
            else:
                with jax.named_scope("_".join(str(v) for v in (step[0],) + step[1])):
                    follow(step)
            n += 1
            continue
        name = step[1]
        count = units[name]
        between = {}
        i = 0
        n += 1
        while i + 1 < count:
            if order[n] == ("unit", name, i + 1):
                i += 1
            else:
                between.setdefault(i, []).append(order[n])
            n += 1
        before, work, after = stages[name]
        with jax.named_scope(name):
            if before is not None:
                before()

            def one(k, _):
                with jax.named_scope("unit"):
                    work(k)
                for at, todo in between.items():

                    @pl.when(k == at)
                    def _():
                        for item in todo:
                            with jax.named_scope("_".join(str(v) for v in ((item[0],) + item[1] if item[0] != "unit" else item))):
                                follow(item)

                return 0

            lax.fori_loop(0, count, one, 0)
            if after is not None:
                after()
    with jax.named_scope("drain"):
        for n in range(max(0, len(sends) - POOL), len(sends)):
            finish(n)


def body(
    activation_sequence,
    rms_multiplier_vector,
    linear_memory_source_matrix,
    linear_memory_exit_matrix,
    filter_exit_mask_matrix,
    filter_entry_mask_matrix,
    filter_source_matrix,
    memory_prefilter_taps,
    filter_taps_depthwise,
    fading_mask_diagonal_tiles,
    entry_mask_diagonal_tiles,
    fading_speed_per_channel,
    speed_multiplier,
    jump_per_position,
    boundary_hidden_vectors,
    final_mixing_matrix,
):
    dma = pltpu.SemaphoreType.DMA
    mixed = pl.pallas_call(
        kernel,
        name="layer",
        out_shape=jax.ShapeDtypeStruct((256, 2, WIDE), bf16),
        in_specs=[pl.BlockSpec(memory_space=pl.ANY)] * 16,
        out_specs=pl.BlockSpec(memory_space=pltpu.VMEM),
        scratch_shapes=[
            pltpu.VMEM((2, STEPS, 4, 2, WIDE), bf16),
            pltpu.VMEM((4, 2, WIDE), bf16),
            pltpu.VMEM((2 * OWN + 32, WIDE), bf16),
            pltpu.VMEM((4, 4, 4, W_END, LANES), bf16),
            pltpu.VMEM((4, 4, 4, 2, OUT_ROWS, LANES), bf16),
            pltpu.VMEM((16, LANES), bf16),
            pltpu.VMEM((4, LANES), bf16),
            pltpu.VMEM((3, LANES), bf16),
            pltpu.VMEM((2, LANES), f32),
            pltpu.VMEM((2, 2, LANES), f32),
            pltpu.VMEM((2, 16, LANES), f32),
            pltpu.VMEM((4, 16, LANES), f32),
            pltpu.VMEM((2, 1024, LANES), f32),
            pltpu.VMEM((2, 2, 544, 256), f32),
            pltpu.VMEM((2, 2, 544, 256), f32),
            pltpu.VMEM((2, 32, 256), f32),
            pltpu.VMEM((2, 2, 2, OWN, 256), f32),
            pltpu.VMEM((2, 2, 2, OWN, 256), f32),
            pltpu.VMEM((2, 2, OWN, 256), f32),
            pltpu.VMEM((2, 2, 4, OWN, LANES), bf16),
            pltpu.VMEM((2, 4, OWN, LANES), bf16),
            pltpu.VMEM((2, 2, 2, 2, 8, 256), f32),
            pltpu.VMEM((3, 2, 2, 2, 8, 256), f32),
            pltpu.VMEM((3, 4, 8, 512), f32),
            dma((18,)),
            dma((16,)),
            dma((POOL,)),
            dma((204,)),
            dma((3, 4)),
            dma((4,)),
            dma((2,)),
            dma((3,)),
            dma((9,)),
            dma((2,)),
        ],
        compiler_params=pltpu.CompilerParams(
            collective_id=0, has_side_effects=True, vmem_limit_bytes=54 * 1024 * 1024
        ),
    )(
        activation_sequence,
        rms_multiplier_vector.reshape(16, LANES),
        linear_memory_source_matrix,
        linear_memory_exit_matrix,
        filter_exit_mask_matrix,
        filter_entry_mask_matrix,
        filter_source_matrix,
        memory_prefilter_taps,
        filter_taps_depthwise,
        fading_mask_diagonal_tiles.reshape(256, LANES),
        entry_mask_diagonal_tiles.reshape(256, LANES),
        fading_speed_per_channel,
        speed_multiplier.reshape(16, LANES),
        jump_per_position.reshape(16, LANES),
        boundary_hidden_vectors,
        final_mixing_matrix.transpose(0, 2, 1),
    )
    return pl.pallas_call(
        hand_over,
        name="hand_over",
        out_shape=jax.ShapeDtypeStruct(mixed.shape, bf16),
        in_specs=[pl.BlockSpec(memory_space=pl.ANY)],
        out_specs=pl.BlockSpec(memory_space=pl.ANY),
        scratch_shapes=[pltpu.VMEM((256, 2, WIDE), bf16), dma((8,)), dma((8,))],
    )(mixed)


def hand_over(src, dst, held, in_sem, out_sem):
    parts = [pl.ds(n * 32, 32) for n in range(8)]
    reads = [pltpu.make_async_copy(src.at[p], held.at[p], in_sem.at[n]) for n, p in enumerate(parts)]
    writes = [pltpu.make_async_copy(held.at[p], dst.at[p], out_sem.at[n]) for n, p in enumerate(parts)]
    for copy in reads:
        copy.start()
    for a, b in zip(reads, writes):
        a.wait()
        b.start()
    for copy in writes:
        copy.wait()


def solution(mesh):
    return jax.shard_map(
        body,
        mesh=mesh,
        in_specs=(
            P(("sp", "tp"), None, None),
            P(),
            P("sp", "tp"),
            P("sp", "tp"),
            P("sp", "tp"),
            P("sp", "tp"),
            P("sp", "tp"),
            P(None, "tp"),
            P(None, "tp"),
            P(None, "tp", None, None),
            P(None, "tp", None, None),
            P(None, "tp"),
            P("sp"),
            P("sp"),
            P(None, None, "tp"),
            P(None, None, ("sp", "tp")),
        ),
        out_specs=P(("sp", "tp"), None, None),
        check_vma=False,
    )
```

```python
import jax
import jax.numpy as jnp
from jax import lax
from jax.experimental import pallas as pl
from jax.experimental.pallas import tpu as pltpu
from jax.sharding import PartitionSpec as P

MESH = pl.DeviceIdType.MESH
f32, bf16 = jnp.float32, jnp.bfloat16

EPS = 1e-06
RING = 4
OWN = 512
STEPS = 64
WIDE = 2048
LANES = 128
POOL = 32

SRC, GATES, CGATE, CIN, COUT, EXIT, W_END = 0, 128, 160, 288, 416, 544, 672
OUT_ROWS = 256

PIECES = (
    ("w", ((0, 64), (64, 112), (112, 160))),
    ("w", ((160, 240), (240, 320), (320, 416))),
    ("w", ((416, 496), (496, 592), (592, 672))),
    ("o", ((0, 80), (80, 160), (160, 256))),
)
FINE = (True, True, True, True)
FAR = ()
ORDERS = (("y", "x", "z"), ("x", "z", "y"), ("z", "y", "x"))
NEAR = (0, -1, 1, 2)
FORWARD = {1: (0, -1), -1: (1, 2)}


def turn_of(piece):
    return 1 if piece % 2 == 0 else -1


def places(piece):
    return 7 if FINE[piece] else 5


def first_place(piece, colour):
    return sum(3 * (3 + 2 * places(p)) for p in range(piece)) + colour * (3 + 2 * places(piece))


def group_of(m):
    piece, colour, phase, kind, way, r = m
    if kind == "pass":
        return (piece, colour, 3, 0, 4)
    if phase == 0:
        return (piece, colour, 0, 2 if kind != "own" else (0 if way == 1 else 1), 1)
    first = 3 + places(piece) * (phase - 1)
    if kind != "own":
        return (piece, colour, phase, first + places(piece) - 1, 4 if FINE[piece] else 2)
    if not FINE[piece]:
        return (piece, colour, phase, first + (r if way == 1 else 3 - r), 1)
    alone = FORWARD[way]
    place = alone.index(r) if r in alone else 2
    return (piece, colour, phase, first + place + (0 if way == 1 else 3), 1 if r in alone else 2)


def messages(piece, colour):
    found = {}
    up = turn_of(piece)
    fine = FINE[piece]

    def one(phase, kind, way, r):
        return (piece, colour, phase, kind, way, r)

    def here(*given):
        return tuple(dict.fromkeys(group_of(m) for m in given))

    def both(phase, r, needs):
        for way in (1, -1):
            found[one(phase, "own", way, r)] = needs

    both(0, 0, ())
    if (piece, 0) in FAR:
        opposite = one(0, "far", up, 0)
        found[opposite] = ()
    else:
        opposite = one(0, "fwd", up, 0)
        found[opposite] = here(one(0, "own", up, 0))
    near = [one(0, "own", 1, 0), one(0, "own", -1, 0)]
    before = here(*near, opposite)
    ready = {0: (), -1: here(near[0]), 1: here(near[1]), 2: here(opposite)}
    for phase in (1, 2):
        for r in NEAR if fine else (0, 1):
            both(phase, r, ready[r] if fine else before)
        last = []
        if (piece, phase) in FAR:
            for r in NEAR:
                last.append(one(phase, "far", up, r))
                found[last[-1]] = ready[r]
        else:
            for way in (1, -1):
                for r in FORWARD[way] if fine else ((0,) if way == 1 else (1,)):
                    last.append(one(phase, "fwd", way, r))
                    found[last[-1]] = here(one(phase, "own", way, r))
        parts = NEAR if fine else (0, 1)
        ready = {
            0: before,
            -1: here(*(one(phase, "own", 1, r) for r in parts)),
            1: here(*(one(phase, "own", -1, r) for r in parts)),
            2: here(*last),
        }
        if phase == 2:
            break
        before = before + ready[-1] + ready[1] + ready[2]
    if PIECES[piece][0] == "o":
        for slot, r in enumerate(NEAR):
            found[one(3, "pass", 0, slot)] = before if r == 0 else ready[r]
    return found


def size(m):
    first, last = PIECES[m[0]][1][m[1]]
    chunks = (1, 1, 4, 16)[m[2]] * (1 if FINE[m[0]] or m[2] in (0, 3) else 2)
    return (last - first) * 0.25 * chunks * (2 if m[3] == "far" else 1)


RATE, HOP = 44.0, 2.8
SIDE_RATE, SIDE_HOP = 450.0, 1.4

STAGES = (
    ("norm_own", 4, 1.55, ()),
    ("norm_other", 4, 1.55, ("rows",)),
    ("norm_edges", 1, 0.3, ("edges",)),
    ("spots", 1, 0.8, ("small",)),
    ("source", 4, 0.78, ("norm_own", "norm_other", "norm_edges", 0)),
    ("source_edges", 1, 0.6, ("source",)),
    ("gates", 2, 1.65, ("source_edges", "spots")),
    ("gates_shake", 4, 1.85, ("gates", 1)),
    ("totals", 1, 1.3, ("gates_shake",)),
    ("hear0", 1, 0.4, ("told0",)),
    ("hear1", 1, 0.4, ("told1",)),
    ("hear2", 1, 0.5, ("told2",)),
    ("shake_edges", 1, 0.8, ("gates_shake",)),
    ("exit_gate", 4, 0.8, (2, "norm_other")),
    ("conv", 4, 0.8, (2, "shake_edges")),
    ("states", 1, 1.5, ("hear2", "exit_gate")),
    ("result", 8, 0.78, (3, "swapped0", "swapped1")),
)
BACKLOG = 1.5


def PRIORITY(m):
    return (m[0], m[2])


def plan():
    deps = {}
    for piece in range(len(PIECES)):
        for colour in range(3):
            deps.update(messages(piece, colour))
    groups = {}
    for m in deps:
        groups.setdefault(group_of(m), []).append(m)
    clock, link, coming, arrive, sent, got = 0.0, {}, {}, {}, set(), set()
    times = {"rows": 6.0, "edges": 4.0, "small": 6.0}
    order, done, progress = [], set(), {}

    def send_ready():
        ready = [m for m in deps if m not in sent and all(d in got for d in deps[m])]
        for m in sorted(ready, key=PRIORITY):
            side = m[3] == "pass"
            wire = "side" if side else (ORDERS[m[1]][m[2]], m[4])
            if link.get(wire, 0.0) - clock > BACKLOG:
                continue
            link[wire] = max(clock, link.get(wire, 0.0)) + size(m) / (SIDE_RATE if side else RATE)
            arrive[m] = link[wire] + (SIDE_HOP if side else HOP + (0.8 if m[3] == "far" else 0.0))
            sent.add(m)
            order.append(("send", m))
            g = group_of(m)
            if all(n in sent for n in groups[g]):
                coming[g] = max(arrive[n] for n in groups[g])

    def met(need):
        if isinstance(need, int):
            return all(g in got for g in groups if g[0] == need)
        return need in done or times.get(need, 1e9) <= clock

    current = None
    send_ready()
    while len(done) < len(STAGES):
        here = sorted((m for m in coming if m not in got and coming[m] <= clock), key=lambda m: (m[0], coming[m]))
        if here:
            m = here[0]
            got.add(m)
            order.append(("wait", m))
            clock += 0.03
            send_ready()
            continue
        send_ready()
        if current is None:
            for n, stage in enumerate(STAGES):
                if stage[0] not in done and all(met(need) for need in stage[3]):
                    current = stage
                    break
        quick = next(
            (st for st in STAGES if st[0].startswith("hear") and st[0] not in done and all(met(k) for k in st[3])), None
        )
        if quick is not None:
            order.append(("unit", quick[0], 0))
            clock += quick[2]
            done.add(quick[0])
            level = int(quick[0][4])
            if level < 2:
                times[f"told{level + 1}"] = clock + 3.5
            if current is quick:
                current = None
            continue
        if current is not None:
            name, units, cost, _ = current
            i = progress.get(name, 0)
            order.append(("unit", name, i))
            clock += cost
            progress[name] = i + 1
            if i + 1 == units:
                done.add(name)
                current = None
                if name == "totals":
                    times["told0"] = clock + 3.5
                if name == "conv":
                    times["swapped1"] = clock + 3.0
                if name == "states":
                    times["swapped0"] = clock + 3.0
            continue
        if any(m not in sent and all(d in got for d in deps[m]) for m in deps):
            clock += 0.25
            continue
        later = [t for m, t in coming.items() if m not in got] + [t for t in times.values() if t > clock]
        clock = min(t for t in later if t > clock)
    return order, clock


def wrap(i):
    return lax.rem(i + RING, RING)


def rows_of(shape):
    return lax.broadcasted_iota(jnp.int32, shape, 0)


def turn(v, by):
    return pltpu.roll(v, by, 0)


def spread(v, first):
    row = rows_of(v.shape)
    v = jnp.where((row >= first) & (row < first + 2), v, 0.0)
    v = v + turn(v, 2)
    return v + turn(v, 4)


def kernel(
    x_in, gain_in, src_in, exit_in, cout_in, cgate_in, cin_in, taps_in, ctaps_in, fade_in, entry_in, speed_in,
    tempo_in, jump_in, edge_in, out_w, out,
    XR, XE, X, G, Wo, GN, TB, CB, SB, BB, PM, SM, MJ, Rp, Sp, Hh, A, U, GL, ACT, ACTS, SEG, PRE, XS, OUT,
    lsem, wsem, pool, grecv, frecv, xrecv, hrecv, srecv, erecv, arecv, osem,
):
    sp, tp = lax.axis_index("sp"), lax.axis_index("tp")
    me = {"z": sp // 4, "x": lax.rem(sp, 4), "y": tp // 2}
    c = lax.rem(tp, 2)
    z, x, y = me["z"], me["x"], me["y"]
    q = sp * 4 + y

    def device(at, core):
        return {"sp": at["z"] * 4 + at["x"], "tp": at["y"] * 2 + core}

    def along(d, by):
        return {**me, d: wrap(me[d] + by)}

    sibling = device(me, 1 - c)
    ahead = lax.rem(q + 1, 64)
    behind = lax.rem(q + 63, 64)

    def chip(number, core):
        return {"sp": number // 4, "tp": lax.rem(number, 4) * 2 + core}

    barrier = pltpu.get_barrier_semaphore()

    def hello(to):
        pl.semaphore_signal(barrier, inc=1, device_id=to, device_id_type=MESH)

    hello(sibling)
    for d in ("z", "x", "y"):
        for by in (1, 2, 3):
            hello(device(along(d, by), c))
    hello(chip(behind, 1))
    hello(chip(ahead, 0))

    def own_rows(first, count):
        return G.at[z, x, y, pl.ds(first, count)]

    sp16 = pl.ds(pl.multiple_of(sp * 16, 16), 16)
    pairs = [
        (src_in, own_rows(SRC, 128)),
        (fade_in.at[sp16], own_rows(GATES, 16)),
        (entry_in.at[sp16], own_rows(GATES + 16, 16)),
        (cgate_in, own_rows(CGATE, 128)),
        (cin_in, own_rows(CIN, 128)),
        (cout_in, own_rows(COUT, 128)),
        (exit_in, own_rows(EXIT, 128)),
        (gain_in, GN),
        (taps_in, TB),
        (ctaps_in, CB),
        (speed_in, SB),
        (edge_in, BB),
        (tempo_in, PM.at[0]),
        (jump_in, PM.at[1]),
    ]
    pairs += [(x_in.at[pl.ds(seg * STEPS, STEPS)], XR.at[c, :, seg]) for seg in range(4)]
    local = [pltpu.make_async_copy(a, b, lsem.at[n]) for n, (a, b) in enumerate(pairs)]
    out_local = [
        pltpu.make_async_copy(
            out_w.at[n // 8, :, pl.ds((n % 8) * LANES, LANES)], Wo.at[z, x, y, c, pl.ds(n * 16, 16)], wsem.at[n]
        )
        for n in range(16)
    ]
    for copy in local + out_local:
        copy.start()
    pl.semaphore_wait(barrier, 12)

    def remote(src, dst, send, recv, to):
        return pltpu.make_async_remote_copy(
            src_ref=src, dst_ref=dst, send_sem=pool.at[0] if send is None else send, recv_sem=recv, device_id=to, device_id_type=MESH
        )

    sends = []

    def go(make, *given):
        n = len(sends)
        if n >= POOL:
            finish(n - POOL)
        make(*given, send=pool.at[n % POOL]).start()
        sends.append((make, given))

    def finish(n):
        make, given = sends[n]
        make(*given, send=pool.at[n % POOL]).wait_send()

    def rows_copy(seg, send=None):
        return remote(
            x_in.at[pl.ds(seg * STEPS, STEPS)], XR.at[c, :, seg], send, xrecv.at[seg], sibling
        )

    target = jnp.where(c == 1, ahead, behind)

    def edge_copy(core, slot, send=None):
        return remote(
            x_in.at[pl.ds(c * 254, 2)], XE.at[pl.ds((1 - c) * 2, 2)], send, hrecv.at[slot], chip(target, core)
        )

    def region(piece, colour, phase, i, r, count=1):
        kind, parts = PIECES[piece]
        first, last = parts[colour]
        a, b, d = ORDERS[colour]
        where = dict(me)
        if phase == 0:
            where[a] = i
        elif phase < 3:
            cut = (a, b)[phase - 1]
            if phase == 2:
                where[a] = slice(None)
            where[(b, d)[phase - 1]] = i
            if FINE[piece]:
                where[cut] = wrap(me[cut] + r) if count == 1 else pl.ds(0, count)
            else:
                where[cut] = pl.ds(2 * r, 2) if count == 1 else slice(None)
        else:
            where[a], where[b] = slice(None), slice(None)
            where[d] = i if count == 1 else slice(None)
        rows = pl.ds(first, last - first)
        if kind == "w":
            return G.at[where["z"], where["x"], where["y"], rows]
        return Wo.at[where["z"], where["x"], where["y"], c, rows]

    def message(m, send=None):
        piece, colour, phase, kind, way, r = m
        if kind == "pass":
            d = ORDERS[colour][2]
            ref = region(piece, colour, 3, wrap(me[d] + NEAR[r]), 0)
            return remote(ref, ref, send, frecv.at[(piece - 3) * 3 + colour], sibling)
        d = ORDERS[colour][phase]
        block = wrap(me[d] - way) if kind == "fwd" else me[d]
        ref = region(piece, colour, phase, block, r)
        at = first_place(piece, colour) + group_of(m)[3]
        return remote(ref, ref, send, grecv.at[at], device(along(d, 2 if kind == "far" else way), c))

    def group_here(g):
        piece, colour, phase, place, count = g
        ref = region(piece, colour, phase, 0, 0, count)
        at = frecv.at[(piece - 3) * 3 + colour] if phase == 3 else grecv.at[first_place(piece, colour) + place]
        remote(ref, ref, None, at, sibling).wait_recv()

    def small_arrays():
        for copy in local[7:14]:
            copy.wait()
        for row in range(4):
            SM[y, row : row + 1, :] = TB[row : row + 1, :].astype(f32)
        for row in range(3):
            SM[y, 4 + row : 5 + row, :] = CB[row : row + 1, :].astype(f32)
        for row in range(2):
            SM[y, 7 + row : 8 + row, :] = SB[row : row + 1, :]
            for b in range(2):
                SM[y, 9 + 2 * row + b : 10 + 2 * row + b, :] = BB[row, b : b + 1, :]
        SM[y, 13:16, :] = jnp.zeros((3, LANES), f32)

    def small_copy(by, send=None):
        return remote(SM.at[y], SM.at[y], send, srecv.at[by - 1], device(along("y", by), c))

    def positions():
        seg = rows_of((8, LANES)) // 2
        for n in range(2):
            for rc in range(2):
                lines = [
                    jnp.broadcast_to(PM[n, pl.ds(4 * y + rc * 2 + k, 1), :], (8, LANES)) for k in range(2)
                ]
                v = jnp.where(
                    seg == 0,
                    lines[0],
                    jnp.where(
                        seg == 1, pltpu.roll(lines[0], 64, 1), jnp.where(seg == 2, lines[1], pltpu.roll(lines[1], 64, 1))
                    ),
                )
                for j in range(STEPS):
                    MJ[n, rc * OWN + j * 8 : rc * OWN + j * 8 + 8, :] = jnp.broadcast_to(v[:, j : j + 1], (8, LANES))

    def scaled(parts, alive=None):
        total = parts[0] * parts[0]
        for v in parts[1:]:
            total = total + v * v
        r = lax.rsqrt(jnp.sum(total, axis=1, keepdims=True) * (1.0 / WIDE) + EPS)
        if alive is not None:
            r = r * alive
        r = jnp.broadcast_to(r, parts[0].shape)
        return [(v * r) * GN[n : n + 1, :].astype(f32) for n, v in enumerate(parts)]

    def norm_unit(rc, i):
        def one(k, _):
            j = i * 16 + k * 2
            parts = [
                XR[rc, pl.ds(j, 2), :, :, n * LANES : (n + 1) * LANES].astype(f32).reshape(16, LANES) for n in range(16)
            ]
            rows = pl.ds(pl.multiple_of(rc * OWN + j * 8, 16), 16)
            for n, v in enumerate(scaled(parts)):
                X[rows, n * LANES : (n + 1) * LANES] = v.astype(bf16)
            return 0

        lax.fori_loop(0, 8, one, 0)

    def norm_edges():
        row = rows_of((8, 1))
        alive = jnp.where(row < 4, jnp.where(q > 0, 1.0, 0.0), jnp.where(q < 63, 1.0, 0.0))
        parts = [XE[:, :, n * LANES : (n + 1) * LANES].astype(f32).reshape(8, LANES) for n in range(16)]
        for n, v in enumerate(scaled(parts, alive)):
            lane = slice(n * LANES, (n + 1) * LANES)
            X[2 * OWN : 2 * OWN + 16, lane] = jnp.concatenate([turn(v, 6), turn(v, 4)], axis=0).astype(bf16)
            X[2 * OWN + 16 : 2 * OWN + 32, lane] = jnp.concatenate([turn(v, 4), turn(v, 4)], axis=0).astype(bf16)

    def weight(row, yp):
        parts = [G[:, :, 2 * yp + h, pl.ds(row, LANES), :].reshape(WIDE, LANES) for h in range(2)]
        return jnp.concatenate(parts, axis=1)

    def project(rows, w):
        return jnp.dot(X[rows, :], w, preferred_element_type=f32)

    def block(work, i):
        yp, rc = i // 2, lax.rem(i, 2)
        work(yp, rc, pl.ds(pl.multiple_of(rc * OWN, OWN), OWN))

    main = pl.ds(16, OWN)
    edges = pl.ds(2 * OWN, 32)

    def pads(Rp):
        for yp in range(2):
            row = rows_of((8, 256))
            for rc in range(2):
                for j in range(2):
                    own = Rp[yp, rc, pl.ds(16 + (STEPS - 2 + j) * 8, 8), :]
                    prior = Hh[yp, pl.ds(8 * j, 8), :] if rc == 0 else Rp[yp, 0, pl.ds(16 + (STEPS - 2 + j) * 8, 8), :]
                    Rp[yp, rc, pl.ds(8 * j, 8), :] = jnp.where(row < 2, turn(prior, 2), turn(own, 2))
                own = Rp[yp, rc, pl.ds(16, 8), :]
                later = Rp[yp, 1, pl.ds(16, 8), :] if rc == 0 else Hh[yp, pl.ds(16, 8), :]
                Rp[yp, rc, pl.ds(16 + OWN, 8), :] = jnp.where(row >= 6, turn(later, 6), turn(own, 6))

    def source(i):
        def work(yp, rc, rows):
            Rp[yp, rc, main, :] = project(rows, weight(SRC, yp))

        block(work, i)

    def source_edges():
        for yp in range(2):
            Hh[yp] = project(edges, weight(SRC, yp))
        pads(Rp)

    def taps(yp, row):
        return jnp.concatenate([SM[2 * yp + h, pl.ds(row, 1), :] for h in range(2)], axis=1)

    GB = 128

    def gates(i):
        def one(k, _):
            gate_rows(0, i, k)
            return 0

        lax.fori_loop(0, 4, one, 0)

    def gate_rows(yp, rc, blk):
        base = pl.multiple_of(blk * GB, GB)
        rc_rows = taps(yp, 0) * Rp[yp, rc, pl.ds(base, GB), :]
        for k in range(1, 4):
            rc_rows = rc_rows + taps(yp, k) * Rp[yp, rc, pl.ds(base + 8 * k, GB), :]
        narrow = (0.5 * rc_rows).astype(bf16)
        half = narrow.astype(f32)
        at = pl.ds(pl.multiple_of(rc * OWN + blk * GB, GB), GB)
        tempo, jump = MJ[0, at, :], MJ[1, at, :]
        for h in range(2):
            lane = slice(h * LANES, (h + 1) * LANES)
            yy = 2 * yp + h
            maps = [
                G[pl.ds(2 * d, 2), :, yy, pl.ds(GATES + 16 * kind, 16), :].reshape(LANES, LANES)
                for kind in range(2)
                for d in range(2)
            ]
            for d in range(2):
                pre = jnp.dot(
                    narrow[:, lane], jnp.concatenate([maps[d], maps[2 + d]], axis=1), preferred_element_type=f32
                )
                speed = SM[yy, pl.ds(7 + d, 1), :] * -4.0
                la = (1.0 + jnp.tanh(pre[:, :LANES])) * (speed * tempo) + jump
                decay = jnp.exp(la)
                near = la * (-2.0 - la * (2.0 + la * (4.0 / 3.0)))
                rest = jnp.where(la > -0.005, near, 1.0 - decay * decay)
                root = rest * lax.rsqrt(jnp.maximum(rest, 1e-36))
                A[d, yp, rc, pl.ds(base, GB), lane] = decay
                U[d, yp, rc, pl.ds(base, GB), lane] = root * (1.0 + jnp.tanh(pre[:, LANES:])) * half[:, lane]

    PAIRS = [(yp, rc) for yp in range(2) for rc in range(2)]

    def tile(ref, d, yp, rc, j):
        return ref[d, yp, rc, pl.ds(pl.multiple_of(j * 8, 8), 8), :]

    def totals():
        def one(i, state):
            new = []
            for d in range(2):
                j = i if d == 0 else STEPS - 1 - i
                for n, (yp, rc) in enumerate(PAIRS):
                    sa, sb = state[d * 4 + n]
                    a = tile(A, d, yp, rc, j)
                    new.append((sa * a, sb * a + tile(U, d, yp, rc, j)))
            return tuple(new)

        start = tuple((jnp.ones((8, 256), f32), jnp.zeros((8, 256), f32)) for _ in range(8))
        end = lax.fori_loop(0, STEPS, one, start)
        row = rows_of((8, 256))
        for yp in range(2):
            whole = []
            for d in range(2):
                ends = []
                for rc in range(2):
                    a, b = end[d * 4 + yp * 2 + rc]
                    for by in (2, 4):
                        shift = by if d == 0 else 8 - by
                        inside = (row >= by) if d == 0 else (row < 8 - by)
                        pa, pb = turn(a, shift), turn(b, shift)
                        b = jnp.where(inside, a * pb + b, b)
                        a = jnp.where(inside, a * pa, a)
                    SEG[d, yp, rc, 0], SEG[d, yp, rc, 1] = a, b
                    ends.append((spread(a, 6 if d == 0 else 0), spread(b, 6 if d == 0 else 0)))
                first, second = ends if d == 0 else ends[::-1]
                whole.append((first[0] * second[0], second[0] * first[1] + second[1]))
            put(0, y, yp, whole)

    def put(level, slot, yp, whole):
        row = rows_of((8, 256))
        (fa, fb), (ba, bb) = whole
        XS[level, slot, :, yp * 256 : (yp + 1) * 256] = jnp.where(
            row < 2, fa, jnp.where(row < 4, fb, jnp.where(row < 6, ba, bb))
        )

    AXES = ("y", "x", "z")

    def share(level, by, send=None):
        d = AXES[level]
        ref = XS.at[level, me[d]]
        k = level * 3 + by - 1
        return remote(ref, ref, send, erecv.at[k], device(along(d, by), c))

    def tell(level):
        for by in (1, 2, 3):
            go(share, level, by)

    def combine(early, late):
        return early[0] * late[0], late[0] * early[1] + late[1]

    def hear(level):
        for by in (1, 2, 3):
            share(level, by).wait_recv()
        m = me[AXES[level]]
        for yp in range(2):
            one = (jnp.ones((8, 256), f32), jnp.zeros((8, 256), f32))
            whole = []
            for d in range(2):
                total, prefix = one, one
                for i in range(4) if d == 0 else range(3, -1, -1):
                    v = XS[level, i, :, yp * 256 : (yp + 1) * 256]
                    item = (spread(v, 4 * d), spread(v, 4 * d + 2))
                    passed = (i < m) if d == 0 else (i > m)
                    longer = combine(prefix, item)
                    prefix = tuple(jnp.where(passed, n, o) for n, o in zip(longer, prefix))
                    total = combine(total, item)
                whole.append(total)
                PRE[level, yp, d, 0], PRE[level, yp, d, 1] = prefix
            if level < 2:
                put(level + 1, me[AXES[level + 1]], yp, whole)
        if level < 2:
            tell(level + 1)

    def entering():
        row = rows_of((8, 256))
        even = (row % 2) == 0
        for yp in range(2):
            for d in range(2):
                h = jnp.where(even, taps(yp, 9 + 2 * d), taps(yp, 10 + 2 * d))
                for level in (2, 1, 0):
                    a, b = PRE[level, yp, d, 0], PRE[level, yp, d, 1]
                    h = a * h + b
                for rc in (0, 1) if d == 0 else (1, 0):
                    a, b = SEG[d, yp, rc, 0], SEG[d, yp, rc, 1]
                    shift = 2 if d == 0 else 6
                    inside = (row >= 2) if d == 0 else (row < 6)
                    pa = jnp.where(inside, turn(a, shift), 1.0)
                    pb = jnp.where(inside, turn(b, shift), 0.0)
                    SEG[d, yp, rc, 0] = pa * h + pb
                    last = 6 if d == 0 else 0
                    h = spread(a, last) * h + spread(b, last)

    def exit_gate(i):
        def work(yp, rc, rows):
            v = project(rows, weight(EXIT, yp))
            inner = v * (0.7978845608028654 + 0.035677408136300125 * v * v)
            GL[yp, rc] = 0.5 * v * (1.0 + jnp.tanh(inner))

        block(work, i)

    def states():
        def forth(i, state):
            new = []
            for n, (yp, rc) in enumerate(PAIRS):
                h = tile(A, 0, yp, rc, i) * state[n] + tile(U, 0, yp, rc, i)
                U[0, yp, rc, pl.ds(pl.multiple_of(i * 8, 8), 8), :] = h
                new.append(h)
            return tuple(new)

        def back(i, state):
            new = []
            low = STEPS - 2 - 2 * i
            rows16 = pl.ds(pl.multiple_of(low * 8, 16), 16)
            for n, (yp, rc) in enumerate(PAIRS):
                h1 = tile(A, 1, yp, rc, low + 1) * state[n] + tile(U, 1, yp, rc, low + 1)
                h0 = tile(A, 1, yp, rc, low) * h1 + tile(U, 1, yp, rc, low)
                both = jnp.concatenate([h0, h1], axis=0) + U[0, yp, rc, rows16, :]
                done = (both * GL[yp, rc, rows16, :]).astype(bf16)
                for h in range(2):
                    ACT[rc, 0, 2 * yp + h, rows16, :] = done[:, h * LANES : (h + 1) * LANES]
                new.append(h0)
            return tuple(new)

        lax.fori_loop(0, STEPS, forth, tuple(SEG[0, yp, rc, 0] for yp, rc in PAIRS))
        lax.fori_loop(0, STEPS // 2, back, tuple(SEG[1, yp, rc, 0] for yp, rc in PAIRS))

    def shake(i):
        def work(yp, rc, rows):
            Sp[yp, rc, main, :] = project(rows, weight(CGATE, yp)) * project(rows, weight(CIN, yp))

        block(work, i)

    def gates_shake(i):
        shake(i)
        for k in range(2):
            gate_rows(1, i // 2, lax.rem(i, 2) * 2 + k)

    def shake_edges():
        for yp in range(2):
            Hh[yp] = project(edges, weight(CGATE, yp)) * project(edges, weight(CIN, yp))
        pads(Sp)

    def conv(i):
        def work(yp, rc, rows):
            v = project(rows, weight(COUT, yp))
            s = jnp.zeros((OWN, 256), f32)
            for k in range(3):
                s = s + taps(yp, 4 + k) * Sp[yp, rc, pl.ds(8 + 8 * k, OWN), :]
            done = (v * s).astype(bf16)
            for h in range(2):
                ACT[rc, 1, 2 * yp + h] = done[:, h * LANES : (h + 1) * LANES]

        block(work, i)

    def swap(m, send=None):
        return remote(ACT.at[1 - c, m], ACTS.at[m], send, arecv.at[m], sibling)

    def result(i):
        zz, xx = i // 2, lax.rem(i, 2) * 2
        left, right = [], []
        for own in range(2):
            core = c if own == 0 else 1 - c
            for m in range(2):
                for yy in range(4):
                    left.append(ACT[c, m, yy] if own == 0 else ACTS[m, yy])
                    k16 = pl.ds(pl.multiple_of((m * 8 + 2 * yy + core) * 16, 16), 16)
                    right.append(Wo[zz, pl.ds(xx, 2), :, :, k16, :].reshape(256, LANES))
        v = lax.dot_general(
            jnp.concatenate(left, axis=1), jnp.concatenate(right, axis=1),
            (((1,), (1,)), ((), ())), preferred_element_type=f32,
        )
        OUT[:, :, :, pl.ds(pl.multiple_of(i * 256, 256), 256)] = v.astype(bf16).reshape(STEPS, 4, 2, 256)

        @pl.when(lax.rem(i, 4) == 3)
        def _():
            for seg in range(4):
                write(i // 4, seg).start()

    def write(i, seg):
        lanes = pl.ds(pl.multiple_of(i * 1024, 1024), 1024)
        return pltpu.make_async_copy(OUT.at[:, seg, :, lanes], out.at[pl.ds(seg * STEPS, STEPS), :, lanes], osem.at[i, seg])

    def before_other():
        for seg in range(4):
            rows_copy(seg).wait_recv()

    def before_edges():
        for slot in range(2):
            edge_copy(0, slot).wait_recv()

    def before_gates():
        for by in (1, 2, 3):
            small_copy(by).wait_recv()
        positions()

    def before_result():
        for m in (1, 0):
            swap(m).wait_recv()

    def after_own():
        for by in (1, 2, 3):
            go(small_copy, by)

    def last_states():
        entering()
        states()

    def await_local():
        for seg in range(4):
            go(rows_copy, seg)
        for core in range(2):
            go(edge_copy, core, 1 - c)
        small_arrays()
        for copy in local[14:]:
            copy.wait()

    stages = {
        "norm_own": (await_local, lambda i: norm_unit(c, i), after_own),
        "norm_other": (before_other, lambda i: norm_unit(1 - c, i), None),
        "norm_edges": (before_edges, lambda i: norm_edges(), None),
        "source": (None, source, None),
        "source_edges": (None, lambda i: source_edges(), None),
        "spots": (None, lambda i: before_gates(), None),
        "gates": (None, gates, None),
        "gates_shake": (None, gates_shake, None),
        "totals": (None, lambda i: totals(), lambda: tell(0)),
        "hear0": (None, lambda i: hear(0), None),
        "hear1": (None, lambda i: hear(1), None),
        "hear2": (None, lambda i: hear(2), None),
        "shake_edges": (None, lambda i: shake_edges(), None),
        "exit_gate": (None, exit_gate, None),
        "conv": (None, conv, lambda: go(swap, 1)),
        "states": (None, lambda i: last_states(), lambda: go(swap, 0)),
        "result": (before_result, result, None),
    }
    held = {0: local[0:3], 1: local[3:5], 2: local[5:7], 3: out_local}
    units = {name: count for name, count, _, _ in STAGES}

    def follow(step):
        if step[0] == "send":
            for copy in held.pop(step[1][0], ()):
                copy.wait()
            go(message, step[1])
        elif step[0] == "wait":
            group_here(step[1])
        else:
            stages[step[1]][1](0)

    order, _ = plan()
    n = 0
    while n < len(order):
        step = order[n]
        if step[0] != "unit" or units[step[1]] == 1:
            if step[0] == "unit":
                before, work, after = stages[step[1]]
                with jax.named_scope(step[1]):
                    if before is not None:
                        before()
                    work(0)
                    if after is not None:
                        after()
            else:
                with jax.named_scope("_".join(str(v) for v in (step[0],) + step[1])):
                    follow(step)
            n += 1
            continue
        name = step[1]
        count = units[name]
        between = {}
        i = 0
        n += 1
        while i + 1 < count:
            if order[n] == ("unit", name, i + 1):
                i += 1
            else:
                between.setdefault(i, []).append(order[n])
            n += 1
        before, work, after = stages[name]
        with jax.named_scope(name):
            if before is not None:
                before()

            def one(k, _):
                with jax.named_scope("unit"):
                    work(k)
                for at, todo in between.items():

                    @pl.when(k == at)
                    def _():
                        for item in todo:
                            with jax.named_scope("_".join(str(v) for v in ((item[0],) + item[1] if item[0] != "unit" else item))):
                                follow(item)

                return 0

            lax.fori_loop(0, count, one, 0)
            if after is not None:
                after()
    for i in range(2):
        for seg in range(4):
            write(i, seg).wait()
    with jax.named_scope("drain"):
        for n in range(max(0, len(sends) - POOL), len(sends)):
            finish(n)


def body(
    activation_sequence,
    rms_multiplier_vector,
    linear_memory_source_matrix,
    linear_memory_exit_matrix,
    filter_exit_mask_matrix,
    filter_entry_mask_matrix,
    filter_source_matrix,
    memory_prefilter_taps,
    filter_taps_depthwise,
    fading_mask_diagonal_tiles,
    entry_mask_diagonal_tiles,
    fading_speed_per_channel,
    speed_multiplier,
    jump_per_position,
    boundary_hidden_vectors,
    final_mixing_matrix,
):
    dma = pltpu.SemaphoreType.DMA
    mixed = pl.pallas_call(
        kernel,
        name="layer",
        out_shape=jax.ShapeDtypeStruct((256, 2, WIDE), bf16),
        in_specs=[pl.BlockSpec(memory_space=pl.ANY)] * 16,
        out_specs=pl.BlockSpec(memory_space=pl.ANY),
        scratch_shapes=[
            pltpu.VMEM((2, STEPS, 4, 2, WIDE), bf16),
            pltpu.VMEM((4, 2, WIDE), bf16),
            pltpu.VMEM((2 * OWN + 32, WIDE), bf16),
            pltpu.VMEM((4, 4, 4, W_END, LANES), bf16),
            pltpu.VMEM((4, 4, 4, 2, OUT_ROWS, LANES), bf16),
            pltpu.VMEM((16, LANES), bf16),
            pltpu.VMEM((4, LANES), bf16),
            pltpu.VMEM((3, LANES), bf16),
            pltpu.VMEM((2, LANES), f32),
            pltpu.VMEM((2, 2, LANES), f32),
            pltpu.VMEM((2, 16, LANES), f32),
            pltpu.VMEM((4, 16, LANES), f32),
            pltpu.VMEM((2, 1024, LANES), f32),
            pltpu.VMEM((2, 2, 544, 256), f32),
            pltpu.VMEM((2, 2, 544, 256), f32),
            pltpu.VMEM((2, 32, 256), f32),
            pltpu.VMEM((2, 2, 2, OWN, 256), f32),
            pltpu.VMEM((2, 2, 2, OWN, 256), f32),
            pltpu.VMEM((2, 2, OWN, 256), f32),
            pltpu.VMEM((2, 2, 4, OWN, LANES), bf16),
            pltpu.VMEM((2, 4, OWN, LANES), bf16),
            pltpu.VMEM((2, 2, 2, 2, 8, 256), f32),
            pltpu.VMEM((3, 2, 2, 2, 8, 256), f32),
            pltpu.VMEM((3, 4, 8, 512), f32),
            pltpu.VMEM((STEPS, 4, 2, WIDE), bf16),
            dma((18,)),
            dma((16,)),
            dma((POOL,)),
            dma((first_place(len(PIECES) - 1, 3),)),
            dma((3,)),
            dma((4,)),
            dma((2,)),
            dma((3,)),
            dma((9,)),
            dma((2,)),
            dma((2, 4)),
        ],
        compiler_params=pltpu.CompilerParams(
            collective_id=0, has_side_effects=True, vmem_limit_bytes=54 * 1024 * 1024
        ),
    )(
        activation_sequence,
        rms_multiplier_vector.reshape(16, LANES),
        linear_memory_source_matrix,
        linear_memory_exit_matrix,
        filter_exit_mask_matrix,
        filter_entry_mask_matrix,
        filter_source_matrix,
        memory_prefilter_taps,
        filter_taps_depthwise,
        fading_mask_diagonal_tiles.reshape(256, LANES),
        entry_mask_diagonal_tiles.reshape(256, LANES),
        fading_speed_per_channel,
        speed_multiplier.reshape(16, LANES),
        jump_per_position.reshape(16, LANES),
        boundary_hidden_vectors,
        final_mixing_matrix.transpose(0, 2, 1),
    )
    return pl.pallas_call(
        hand_over,
        name="hand_over",
        out_shape=jax.ShapeDtypeStruct(mixed.shape, bf16),
        in_specs=[pl.BlockSpec(memory_space=pl.ANY)],
        out_specs=pl.BlockSpec(memory_space=pl.ANY),
        scratch_shapes=[pltpu.VMEM((256, 2, WIDE), bf16), dma((8,)), dma((8,))],
    )(mixed)


def hand_over(src, dst, held, in_sem, out_sem):
    parts = [pl.ds(n * 32, 32) for n in range(8)]
    reads = [pltpu.make_async_copy(src.at[p], held.at[p], in_sem.at[n]) for n, p in enumerate(parts)]
    writes = [pltpu.make_async_copy(held.at[p], dst.at[p], out_sem.at[n]) for n, p in enumerate(parts)]
    for copy in reads:
        copy.start()
    for a, b in zip(reads, writes):
        a.wait()
        b.start()
    for copy in writes:
        copy.wait()


def solution(mesh):
    return jax.shard_map(
        body,
        mesh=mesh,
        in_specs=(
            P(("sp", "tp"), None, None),
            P(),
            P("sp", "tp"),
            P("sp", "tp"),
            P("sp", "tp"),
            P("sp", "tp"),
            P("sp", "tp"),
            P(None, "tp"),
            P(None, "tp"),
            P(None, "tp", None, None),
            P(None, "tp", None, None),
            P(None, "tp"),
            P("sp"),
            P("sp"),
            P(None, None, "tp"),
            P(None, None, ("sp", "tp")),
        ),
        out_specs=P(("sp", "tp"), None, None),
        check_vma=False,
    )
```

```python
import jax
import jax.numpy as jnp
from jax import lax
from jax.experimental import pallas as pl
from jax.experimental.pallas import tpu as pltpu
from jax.sharding import PartitionSpec as P

MESH = pl.DeviceIdType.MESH
f32, bf16 = jnp.float32, jnp.bfloat16

EPS = 1e-06
RING = 4
OWN = 512
STEPS = 64
WIDE = 2048
LANES = 128
POOL = 48

SRC, GATES, CGATE, CIN, COUT, EXIT, W_END = 0, 128, 160, 288, 416, 544, 672
OUT_ROWS = 256

PIECES = (
    ("w", ((0, 64), (64, 112), (112, 160))),
    ("w", ((160, 240), (240, 320), (320, 416))),
    ("w", ((416, 496), (496, 592), (592, 672))),
    ("o", ((0, 80), (80, 160), (160, 256))),
)
FINE = (True, True, True, True)
FAR = ()
ORDERS = (("y", "x", "z"), ("x", "z", "y"), ("z", "y", "x"))
NEAR = (0, -1, 1, 2)
FORWARD = {1: (0, -1), -1: (1, 2)}


def turn_of(piece):
    return 1 if piece % 2 == 0 else -1


def places(piece):
    return 7 if FINE[piece] else 5


def first_place(piece, colour):
    return sum(3 * (3 + 2 * places(p)) for p in range(piece)) + colour * (3 + 2 * places(piece))


def group_of(m):
    piece, colour, phase, kind, way, r = m
    if kind == "pass":
        return (piece, colour, 3, 0, 4)
    if phase == 0:
        return (piece, colour, 0, 2 if kind != "own" else (0 if way == 1 else 1), 1)
    first = 3 + places(piece) * (phase - 1)
    if kind != "own":
        return (piece, colour, phase, first + places(piece) - 1, 4 if FINE[piece] else 2)
    if not FINE[piece]:
        return (piece, colour, phase, first + (r if way == 1 else 3 - r), 1)
    alone = FORWARD[way]
    place = alone.index(r) if r in alone else 2
    return (piece, colour, phase, first + place + (0 if way == 1 else 3), 1 if r in alone else 2)


def messages(piece, colour):
    found = {}
    up = turn_of(piece)
    fine = FINE[piece]

    def one(phase, kind, way, r):
        return (piece, colour, phase, kind, way, r)

    def here(*given):
        return tuple(dict.fromkeys(group_of(m) for m in given))

    def both(phase, r, needs):
        for way in (1, -1):
            found[one(phase, "own", way, r)] = needs

    both(0, 0, ())
    if (piece, 0) in FAR:
        opposite = one(0, "far", up, 0)
        found[opposite] = ()
    else:
        opposite = one(0, "fwd", up, 0)
        found[opposite] = here(one(0, "own", up, 0))
    near = [one(0, "own", 1, 0), one(0, "own", -1, 0)]
    before = here(*near, opposite)
    ready = {0: (), -1: here(near[0]), 1: here(near[1]), 2: here(opposite)}
    for phase in (1, 2):
        for r in NEAR if fine else (0, 1):
            both(phase, r, ready[r] if fine else before)
        last = []
        if (piece, phase) in FAR:
            for r in NEAR:
                last.append(one(phase, "far", up, r))
                found[last[-1]] = ready[r]
        else:
            for way in (1, -1):
                for r in FORWARD[way] if fine else ((0,) if way == 1 else (1,)):
                    last.append(one(phase, "fwd", way, r))
                    found[last[-1]] = here(one(phase, "own", way, r))
        parts = NEAR if fine else (0, 1)
        ready = {
            0: before,
            -1: here(*(one(phase, "own", 1, r) for r in parts)),
            1: here(*(one(phase, "own", -1, r) for r in parts)),
            2: here(*last),
        }
        if phase == 2:
            break
        before = before + ready[-1] + ready[1] + ready[2]
    if PIECES[piece][0] == "o":
        for slot, r in enumerate(NEAR):
            found[one(3, "pass", 0, slot)] = before if r == 0 else ready[r]
    return found


def size(m):
    first, last = PIECES[m[0]][1][m[1]]
    chunks = (1, 1, 4, 16)[m[2]] * (1 if FINE[m[0]] or m[2] in (0, 3) else 2)
    return (last - first) * 0.25 * chunks * (2 if m[3] == "far" else 1)


RATE, HOP = 44.0, 2.8
SIDE_RATE, SIDE_HOP = 450.0, 1.4

STAGES = (
    ("norm_own", 4, 1.55, ()),
    ("norm_other", 4, 1.55, ("rows",)),
    ("norm_edges", 1, 0.3, ("edges",)),
    ("spots", 1, 0.8, ("small",)),
    ("source", 4, 0.78, ("norm_own", "norm_other", "norm_edges", 0)),
    ("source_edges", 1, 0.6, ("source",)),
    ("gates", 2, 1.65, ("source_edges", "spots")),
    ("gates_shake", 4, 1.85, ("gates", 1)),
    ("totals", 1, 1.3, ("gates_shake",)),
    ("hear0", 1, 0.4, ("told0",)),
    ("hear1", 1, 0.4, ("told1",)),
    ("hear2", 1, 0.5, ("told2",)),
    ("shake_edges", 1, 0.8, ("gates_shake",)),
    ("exit_gate", 2, 1.5, (2, "norm_other")),
    ("conv", 2, 1.5, (2, "shake_edges")),
    ("states", 1, 1.5, ("hear2", "exit_gate")),
    ("result", 4, 1.5, (3, "swapped0", "swapped1")),
)
BACKLOG = 1.5


def PRIORITY(m):
    return (m[0], m[2])


def plan():
    deps = {}
    for piece in range(len(PIECES)):
        for colour in range(3):
            deps.update(messages(piece, colour))
    groups = {}
    for m in deps:
        groups.setdefault(group_of(m), []).append(m)
    clock, link, coming, arrive, sent, got = 0.0, {}, {}, {}, set(), set()
    times = {"rows": 6.0, "edges": 4.0, "small": 6.0}
    order, done, progress = [], set(), {}

    def send_ready():
        ready = [m for m in deps if m not in sent and all(d in got for d in deps[m])]
        for m in sorted(ready, key=PRIORITY):
            side = m[3] == "pass"
            wire = "side" if side else (ORDERS[m[1]][m[2]], m[4])
            if link.get(wire, 0.0) - clock > BACKLOG:
                continue
            link[wire] = max(clock, link.get(wire, 0.0)) + size(m) / (SIDE_RATE if side else RATE)
            arrive[m] = link[wire] + (SIDE_HOP if side else HOP + (0.8 if m[3] == "far" else 0.0))
            sent.add(m)
            order.append(("send", m))
            g = group_of(m)
            if all(n in sent for n in groups[g]):
                coming[g] = max(arrive[n] for n in groups[g])

    def met(need):
        if isinstance(need, int):
            return all(g in got for g in groups if g[0] == need)
        return need in done or times.get(need, 1e9) <= clock

    current = None
    send_ready()
    while len(done) < len(STAGES):
        here = sorted((m for m in coming if m not in got and coming[m] <= clock), key=lambda m: (m[0], coming[m]))
        if here:
            m = here[0]
            got.add(m)
            order.append(("wait", m))
            clock += 0.03
            send_ready()
            continue
        send_ready()
        if current is None:
            for n, stage in enumerate(STAGES):
                if stage[0] not in done and all(met(need) for need in stage[3]):
                    current = stage
                    break
        quick = next(
            (st for st in STAGES if st[0].startswith("hear") and st[0] not in done and all(met(k) for k in st[3])), None
        )
        if quick is not None:
            order.append(("unit", quick[0], 0))
            clock += quick[2]
            done.add(quick[0])
            level = int(quick[0][4])
            if level < 2:
                times[f"told{level + 1}"] = clock + 3.5
            if current is quick:
                current = None
            continue
        if current is not None:
            name, units, cost, _ = current
            i = progress.get(name, 0)
            order.append(("unit", name, i))
            clock += cost
            progress[name] = i + 1
            if i + 1 == units:
                done.add(name)
                current = None
                if name == "totals":
                    times["told0"] = clock + 3.5
                if name == "conv":
                    times["swapped1"] = clock + 3.0
                if name == "states":
                    times["swapped0"] = clock + 3.0
            continue
        if any(m not in sent and all(d in got for d in deps[m]) for m in deps):
            clock += 0.25
            continue
        later = [t for m, t in coming.items() if m not in got] + [t for t in times.values() if t > clock]
        clock = min(t for t in later if t > clock)
    return order, clock


def wrap(i):
    return lax.rem(i + RING, RING)


def rows_of(shape):
    return lax.broadcasted_iota(jnp.int32, shape, 0)


def turn(v, by):
    return pltpu.roll(v, by, 0)


def spread(v, first):
    row = rows_of(v.shape)
    v = jnp.where((row >= first) & (row < first + 2), v, 0.0)
    v = v + turn(v, 2)
    return v + turn(v, 4)


def kernel(
    x_in, gain_in, src_in, exit_in, cout_in, cgate_in, cin_in, taps_in, ctaps_in, fade_in, entry_in, speed_in,
    tempo_in, jump_in, edge_in, out_w, out,
    XR, XE, X, G, Wo, GN, TB, CB, SB, BB, PM, SM, MJ, Rp, Sp, Hh, A, U, GL, ACT, ACTS, SEG, PRE, XS, OUT,
    lsem, wsem, pool, grecv, frecv, xrecv, hrecv, srecv, erecv, arecv, osem,
):
    sp, tp = lax.axis_index("sp"), lax.axis_index("tp")
    me = {"z": sp // 4, "x": lax.rem(sp, 4), "y": tp // 2}
    c = lax.rem(tp, 2)
    z, x, y = me["z"], me["x"], me["y"]
    q = sp * 4 + y

    def device(at, core):
        return {"sp": at["z"] * 4 + at["x"], "tp": at["y"] * 2 + core}

    def along(d, by):
        return {**me, d: wrap(me[d] + by)}

    sibling = device(me, 1 - c)
    ahead = lax.rem(q + 1, 64)
    behind = lax.rem(q + 63, 64)

    def chip(number, core):
        return {"sp": number // 4, "tp": lax.rem(number, 4) * 2 + core}

    barrier = pltpu.get_barrier_semaphore()

    def hello(to):
        pl.semaphore_signal(barrier, inc=1, device_id=to, device_id_type=MESH)

    hello(sibling)
    for d in ("z", "x", "y"):
        for by in (1, 2, 3):
            hello(device(along(d, by), c))
    hello(chip(behind, 1))
    hello(chip(ahead, 0))

    def own_rows(first, count):
        return G.at[z, x, y, pl.ds(first, count)]

    sp16 = pl.ds(pl.multiple_of(sp * 16, 16), 16)
    pairs = [
        (src_in, own_rows(SRC, 128)),
        (fade_in.at[sp16], own_rows(GATES, 16)),
        (entry_in.at[sp16], own_rows(GATES + 16, 16)),
        (cgate_in, own_rows(CGATE, 128)),
        (cin_in, own_rows(CIN, 128)),
        (cout_in, own_rows(COUT, 128)),
        (exit_in, own_rows(EXIT, 128)),
        (gain_in, GN),
        (taps_in, TB),
        (ctaps_in, CB),
        (speed_in, SB),
        (edge_in, BB),
        (tempo_in, PM.at[0]),
        (jump_in, PM.at[1]),
    ]
    pairs += [(x_in.at[pl.ds(seg * STEPS, STEPS)], XR.at[c, :, seg]) for seg in range(4)]
    local = [pltpu.make_async_copy(a, b, lsem.at[n]) for n, (a, b) in enumerate(pairs)]
    out_local = [
        pltpu.make_async_copy(
            out_w.at[n // 8, :, pl.ds((n % 8) * LANES, LANES)], Wo.at[z, x, y, c, pl.ds(n * 16, 16)], wsem.at[n]
        )
        for n in range(16)
    ]
    for copy in local + out_local:
        copy.start()
    pl.semaphore_wait(barrier, 12)

    def remote(src, dst, send, recv, to):
        return pltpu.make_async_remote_copy(
            src_ref=src, dst_ref=dst, send_sem=pool.at[0] if send is None else send, recv_sem=recv, device_id=to, device_id_type=MESH
        )

    sends = []

    def go(make, *given):
        n = len(sends)
        if n >= POOL:
            finish(n - POOL)
        make(*given, send=pool.at[n % POOL]).start()
        sends.append((make, given))

    def finish(n):
        make, given = sends[n]
        make(*given, send=pool.at[n % POOL]).wait_send()

    def rows_copy(seg, send=None):
        return remote(
            x_in.at[pl.ds(seg * STEPS, STEPS)], XR.at[c, :, seg], send, xrecv.at[seg], sibling
        )

    target = jnp.where(c == 1, ahead, behind)

    def edge_copy(core, slot, send=None):
        return remote(
            x_in.at[pl.ds(c * 254, 2)], XE.at[pl.ds((1 - c) * 2, 2)], send, hrecv.at[slot], chip(target, core)
        )

    def region(piece, colour, phase, i, r, count=1):
        kind, parts = PIECES[piece]
        first, last = parts[colour]
        a, b, d = ORDERS[colour]
        where = dict(me)
        if phase == 0:
            where[a] = i
        elif phase < 3:
            cut = (a, b)[phase - 1]
            if phase == 2:
                where[a] = slice(None)
            where[(b, d)[phase - 1]] = i
            if FINE[piece]:
                where[cut] = wrap(me[cut] + r) if count == 1 else pl.ds(0, count)
            else:
                where[cut] = pl.ds(2 * r, 2) if count == 1 else slice(None)
        else:
            where[a], where[b] = slice(None), slice(None)
            where[d] = i if count == 1 else slice(None)
        rows = pl.ds(first, last - first)
        if kind == "w":
            return G.at[where["z"], where["x"], where["y"], rows]
        return Wo.at[where["z"], where["x"], where["y"], c, rows]

    def message(m, send=None):
        piece, colour, phase, kind, way, r = m
        if kind == "pass":
            d = ORDERS[colour][2]
            ref = region(piece, colour, 3, wrap(me[d] + NEAR[r]), 0)
            return remote(ref, ref, send, frecv.at[(piece - 3) * 3 + colour], sibling)
        d = ORDERS[colour][phase]
        block = wrap(me[d] - way) if kind == "fwd" else me[d]
        ref = region(piece, colour, phase, block, r)
        at = first_place(piece, colour) + group_of(m)[3]
        return remote(ref, ref, send, grecv.at[at], device(along(d, 2 if kind == "far" else way), c))

    def group_here(g):
        piece, colour, phase, place, count = g
        ref = region(piece, colour, phase, 0, 0, count)
        at = frecv.at[(piece - 3) * 3 + colour] if phase == 3 else grecv.at[first_place(piece, colour) + place]
        remote(ref, ref, None, at, sibling).wait_recv()

    def small_arrays():
        for copy in local[7:14]:
            copy.wait()
        for row in range(4):
            SM[y, row : row + 1, :] = TB[row : row + 1, :].astype(f32)
        for row in range(3):
            SM[y, 4 + row : 5 + row, :] = CB[row : row + 1, :].astype(f32)
        for row in range(2):
            SM[y, 7 + row : 8 + row, :] = SB[row : row + 1, :]
            for b in range(2):
                SM[y, 9 + 2 * row + b : 10 + 2 * row + b, :] = BB[row, b : b + 1, :]
        SM[y, 13:16, :] = jnp.zeros((3, LANES), f32)

    def small_copy(by, send=None):
        return remote(SM.at[y], SM.at[y], send, srecv.at[by - 1], device(along("y", by), c))

    def positions():
        seg = rows_of((8, LANES)) // 2
        for n in range(2):
            for rc in range(2):
                lines = [
                    jnp.broadcast_to(PM[n, pl.ds(4 * y + rc * 2 + k, 1), :], (8, LANES)) for k in range(2)
                ]
                v = jnp.where(
                    seg == 0,
                    lines[0],
                    jnp.where(
                        seg == 1, pltpu.roll(lines[0], 64, 1), jnp.where(seg == 2, lines[1], pltpu.roll(lines[1], 64, 1))
                    ),
                )
                for j in range(STEPS):
                    MJ[n, rc * OWN + j * 8 : rc * OWN + j * 8 + 8, :] = jnp.broadcast_to(v[:, j : j + 1], (8, LANES))

    def scaled(parts, alive=None):
        total = parts[0] * parts[0]
        for v in parts[1:]:
            total = total + v * v
        r = lax.rsqrt(jnp.sum(total, axis=1, keepdims=True) * (1.0 / WIDE) + EPS)
        if alive is not None:
            r = r * alive
        r = jnp.broadcast_to(r, parts[0].shape)
        return [(v * r) * GN[n : n + 1, :].astype(f32) for n, v in enumerate(parts)]

    def norm_unit(rc, i):
        def one(k, _):
            j = i * 16 + k * 2
            parts = [
                XR[rc, pl.ds(j, 2), :, :, n * LANES : (n + 1) * LANES].astype(f32).reshape(16, LANES) for n in range(16)
            ]
            rows = pl.ds(pl.multiple_of(rc * OWN + j * 8, 16), 16)
            for n, v in enumerate(scaled(parts)):
                X[rows, n * LANES : (n + 1) * LANES] = v.astype(bf16)
            return 0

        lax.fori_loop(0, 8, one, 0)

    def norm_edges():
        row = rows_of((8, 1))
        alive = jnp.where(row < 4, jnp.where(q > 0, 1.0, 0.0), jnp.where(q < 63, 1.0, 0.0))
        parts = [XE[:, :, n * LANES : (n + 1) * LANES].astype(f32).reshape(8, LANES) for n in range(16)]
        for n, v in enumerate(scaled(parts, alive)):
            lane = slice(n * LANES, (n + 1) * LANES)
            X[2 * OWN : 2 * OWN + 16, lane] = jnp.concatenate([turn(v, 6), turn(v, 4)], axis=0).astype(bf16)
            X[2 * OWN + 16 : 2 * OWN + 32, lane] = jnp.concatenate([turn(v, 4), turn(v, 4)], axis=0).astype(bf16)

    def weight(row, yp):
        parts = [G[:, :, 2 * yp + h, pl.ds(row, LANES), :].reshape(WIDE, LANES) for h in range(2)]
        return jnp.concatenate(parts, axis=1)

    def project(rows, w):
        return jnp.dot(X[rows, :], w, preferred_element_type=f32)

    def wide(work, i):
        w = jnp.concatenate([G[:, :, y4, pl.ds(work[0], LANES), :].reshape(WIDE, LANES) for y4 in range(4)], axis=1)
        v = project(pl.ds(pl.multiple_of(i * OWN, OWN), OWN), w)
        for yp in range(2):
            work[1](yp, i, v[:, yp * 256 : (yp + 1) * 256])

    def block(work, i):
        yp, rc = i // 2, lax.rem(i, 2)
        work(yp, rc, pl.ds(pl.multiple_of(rc * OWN, OWN), OWN))

    main = pl.ds(16, OWN)
    edges = pl.ds(2 * OWN, 32)

    def pads(Rp):
        for yp in range(2):
            row = rows_of((8, 256))
            for rc in range(2):
                for j in range(2):
                    own = Rp[yp, rc, pl.ds(16 + (STEPS - 2 + j) * 8, 8), :]
                    prior = Hh[yp, pl.ds(8 * j, 8), :] if rc == 0 else Rp[yp, 0, pl.ds(16 + (STEPS - 2 + j) * 8, 8), :]
                    Rp[yp, rc, pl.ds(8 * j, 8), :] = jnp.where(row < 2, turn(prior, 2), turn(own, 2))
                own = Rp[yp, rc, pl.ds(16, 8), :]
                later = Rp[yp, 1, pl.ds(16, 8), :] if rc == 0 else Hh[yp, pl.ds(16, 8), :]
                Rp[yp, rc, pl.ds(16 + OWN, 8), :] = jnp.where(row >= 6, turn(later, 6), turn(own, 6))

    def source(i):
        def work(yp, rc, rows):
            Rp[yp, rc, main, :] = project(rows, weight(SRC, yp))

        block(work, i)

    def source_edges():
        for yp in range(2):
            Hh[yp] = project(edges, weight(SRC, yp))
        pads(Rp)

    def taps(yp, row):
        return jnp.concatenate([SM[2 * yp + h, pl.ds(row, 1), :] for h in range(2)], axis=1)

    GB = 128

    def gates(i):
        def one(k, _):
            gate_rows(0, i, k)
            return 0

        lax.fori_loop(0, 4, one, 0)

    def gate_rows(yp, rc, blk):
        base = pl.multiple_of(blk * GB, GB)
        rc_rows = taps(yp, 0) * Rp[yp, rc, pl.ds(base, GB), :]
        for k in range(1, 4):
            rc_rows = rc_rows + taps(yp, k) * Rp[yp, rc, pl.ds(base + 8 * k, GB), :]
        narrow = (0.5 * rc_rows).astype(bf16)
        half = narrow.astype(f32)
        at = pl.ds(pl.multiple_of(rc * OWN + blk * GB, GB), GB)
        tempo, jump = MJ[0, at, :], MJ[1, at, :]
        for h in range(2):
            lane = slice(h * LANES, (h + 1) * LANES)
            yy = 2 * yp + h
            maps = [
                G[pl.ds(2 * d, 2), :, yy, pl.ds(GATES + 16 * kind, 16), :].reshape(LANES, LANES)
                for kind in range(2)
                for d in range(2)
            ]
            for d in range(2):
                pre = jnp.dot(
                    narrow[:, lane], jnp.concatenate([maps[d], maps[2 + d]], axis=1), preferred_element_type=f32
                )
                speed = SM[yy, pl.ds(7 + d, 1), :] * -4.0
                la = (1.0 + jnp.tanh(pre[:, :LANES])) * (speed * tempo) + jump
                decay = jnp.exp(la)
                near = la * (-2.0 - la * (2.0 + la * (4.0 / 3.0)))
                rest = jnp.where(la > -0.005, near, 1.0 - decay * decay)
                root = rest * lax.rsqrt(jnp.maximum(rest, 1e-36))
                A[d, yp, rc, pl.ds(base, GB), lane] = decay
                U[d, yp, rc, pl.ds(base, GB), lane] = root * (1.0 + jnp.tanh(pre[:, LANES:])) * half[:, lane]

    PAIRS = [(yp, rc) for yp in range(2) for rc in range(2)]

    def tile(ref, d, yp, rc, j):
        return ref[d, yp, rc, pl.ds(pl.multiple_of(j * 8, 8), 8), :]

    def totals():
        def one(i, state):
            new = []
            for d in range(2):
                j = i if d == 0 else STEPS - 1 - i
                for n, (yp, rc) in enumerate(PAIRS):
                    sa, sb = state[d * 4 + n]
                    a = tile(A, d, yp, rc, j)
                    new.append((sa * a, sb * a + tile(U, d, yp, rc, j)))
            return tuple(new)

        start = tuple((jnp.ones((8, 256), f32), jnp.zeros((8, 256), f32)) for _ in range(8))
        end = lax.fori_loop(0, STEPS, one, start)
        row = rows_of((8, 256))
        for yp in range(2):
            whole = []
            for d in range(2):
                ends = []
                for rc in range(2):
                    a, b = end[d * 4 + yp * 2 + rc]
                    for by in (2, 4):
                        shift = by if d == 0 else 8 - by
                        inside = (row >= by) if d == 0 else (row < 8 - by)
                        pa, pb = turn(a, shift), turn(b, shift)
                        b = jnp.where(inside, a * pb + b, b)
                        a = jnp.where(inside, a * pa, a)
                    SEG[d, yp, rc, 0], SEG[d, yp, rc, 1] = a, b
                    ends.append((spread(a, 6 if d == 0 else 0), spread(b, 6 if d == 0 else 0)))
                first, second = ends if d == 0 else ends[::-1]
                whole.append((first[0] * second[0], second[0] * first[1] + second[1]))
            put(0, y, yp, whole)

    def put(level, slot, yp, whole):
        row = rows_of((8, 256))
        (fa, fb), (ba, bb) = whole
        XS[level, slot, :, yp * 256 : (yp + 1) * 256] = jnp.where(
            row < 2, fa, jnp.where(row < 4, fb, jnp.where(row < 6, ba, bb))
        )

    AXES = ("y", "x", "z")

    def share(level, by, send=None):
        d = AXES[level]
        ref = XS.at[level, me[d]]
        k = level * 3 + by - 1
        return remote(ref, ref, send, erecv.at[k], device(along(d, by), c))

    def tell(level):
        for by in (1, 2, 3):
            go(share, level, by)

    def combine(early, late):
        return early[0] * late[0], late[0] * early[1] + late[1]

    def hear(level):
        for by in (1, 2, 3):
            share(level, by).wait_recv()
        m = me[AXES[level]]
        for yp in range(2):
            one = (jnp.ones((8, 256), f32), jnp.zeros((8, 256), f32))
            whole = []
            for d in range(2):
                total, prefix = one, one
                for i in range(4) if d == 0 else range(3, -1, -1):
                    v = XS[level, i, :, yp * 256 : (yp + 1) * 256]
                    item = (spread(v, 4 * d), spread(v, 4 * d + 2))
                    passed = (i < m) if d == 0 else (i > m)
                    longer = combine(prefix, item)
                    prefix = tuple(jnp.where(passed, n, o) for n, o in zip(longer, prefix))
                    total = combine(total, item)
                whole.append(total)
                PRE[level, yp, d, 0], PRE[level, yp, d, 1] = prefix
            if level < 2:
                put(level + 1, me[AXES[level + 1]], yp, whole)
        if level < 2:
            tell(level + 1)

    def entering():
        row = rows_of((8, 256))
        even = (row % 2) == 0
        for yp in range(2):
            for d in range(2):
                h = jnp.where(even, taps(yp, 9 + 2 * d), taps(yp, 10 + 2 * d))
                for level in (2, 1, 0):
                    a, b = PRE[level, yp, d, 0], PRE[level, yp, d, 1]
                    h = a * h + b
                for rc in (0, 1) if d == 0 else (1, 0):
                    a, b = SEG[d, yp, rc, 0], SEG[d, yp, rc, 1]
                    shift = 2 if d == 0 else 6
                    inside = (row >= 2) if d == 0 else (row < 6)
                    pa = jnp.where(inside, turn(a, shift), 1.0)
                    pb = jnp.where(inside, turn(b, shift), 0.0)
                    SEG[d, yp, rc, 0] = pa * h + pb
                    last = 6 if d == 0 else 0
                    h = spread(a, last) * h + spread(b, last)

    def exit_gate(i):
        def work(yp, rc, v):
            inner = v * (0.7978845608028654 + 0.035677408136300125 * v * v)
            GL[yp, rc] = 0.5 * v * (1.0 + jnp.tanh(inner))

        wide((EXIT, work), i)

    def states():
        def forth(i, state):
            new = []
            for n, (yp, rc) in enumerate(PAIRS):
                h = tile(A, 0, yp, rc, i) * state[n] + tile(U, 0, yp, rc, i)
                U[0, yp, rc, pl.ds(pl.multiple_of(i * 8, 8), 8), :] = h
                new.append(h)
            return tuple(new)

        def back(i, state):
            new = []
            low = STEPS - 2 - 2 * i
            rows16 = pl.ds(pl.multiple_of(low * 8, 16), 16)
            for n, (yp, rc) in enumerate(PAIRS):
                h1 = tile(A, 1, yp, rc, low + 1) * state[n] + tile(U, 1, yp, rc, low + 1)
                h0 = tile(A, 1, yp, rc, low) * h1 + tile(U, 1, yp, rc, low)
                both = jnp.concatenate([h0, h1], axis=0) + U[0, yp, rc, rows16, :]
                done = (both * GL[yp, rc, rows16, :]).astype(bf16)
                for h in range(2):
                    ACT[rc, 0, 2 * yp + h, rows16, :] = done[:, h * LANES : (h + 1) * LANES]
                new.append(h0)
            return tuple(new)

        lax.fori_loop(0, STEPS, forth, tuple(SEG[0, yp, rc, 0] for yp, rc in PAIRS))
        lax.fori_loop(0, STEPS // 2, back, tuple(SEG[1, yp, rc, 0] for yp, rc in PAIRS))

    def shake(i):
        def work(yp, rc, rows):
            Sp[yp, rc, main, :] = project(rows, weight(CGATE, yp)) * project(rows, weight(CIN, yp))

        block(work, i)

    def gates_shake(i):
        shake(i)
        for k in range(2):
            gate_rows(1, i // 2, lax.rem(i, 2) * 2 + k)

    def shake_edges():
        for yp in range(2):
            Hh[yp] = project(edges, weight(CGATE, yp)) * project(edges, weight(CIN, yp))
        pads(Sp)

    def conv(i):
        def work(yp, rc, v):
            s = jnp.zeros((OWN, 256), f32)
            for k in range(3):
                s = s + taps(yp, 4 + k) * Sp[yp, rc, pl.ds(8 + 8 * k, OWN), :]
            done = (v * s).astype(bf16)
            for h in range(2):
                ACT[rc, 1, 2 * yp + h] = done[:, h * LANES : (h + 1) * LANES]

        wide((COUT, work), i)

    def swap(m, send=None):
        return remote(ACT.at[1 - c, m], ACTS.at[m], send, arecv.at[m], sibling)

    def result(i):
        zz = i
        left, right = [], []
        for own in range(2):
            core = c if own == 0 else 1 - c
            for m in range(2):
                for yy in range(4):
                    left.append(ACT[c, m, yy] if own == 0 else ACTS[m, yy])
                    k16 = pl.ds(pl.multiple_of((m * 8 + 2 * yy + core) * 16, 16), 16)
                    right.append(Wo[zz, :, :, :, k16, :].reshape(512, LANES))
        v = lax.dot_general(
            jnp.concatenate(left, axis=1), jnp.concatenate(right, axis=1),
            (((1,), (1,)), ((), ())), preferred_element_type=f32,
        )
        OUT[:, :, :, pl.ds(pl.multiple_of(i * 512, 512), 512)] = v.astype(bf16).reshape(STEPS, 4, 2, 512)

        @pl.when(lax.rem(i, 2) == 1)
        def _():
            for seg in range(4):
                write(i // 2, seg).start()

    def write(i, seg):
        lanes = pl.ds(pl.multiple_of(i * 1024, 1024), 1024)
        return pltpu.make_async_copy(OUT.at[:, seg, :, lanes], out.at[pl.ds(seg * STEPS, STEPS), :, lanes], osem.at[i, seg])

    def before_other():
        for seg in range(4):
            rows_copy(seg).wait_recv()

    def before_edges():
        for slot in range(2):
            edge_copy(0, slot).wait_recv()

    def before_gates():
        for by in (1, 2, 3):
            small_copy(by).wait_recv()
        positions()

    def before_result():
        for m in (1, 0):
            swap(m).wait_recv()

    def after_own():
        for by in (1, 2, 3):
            go(small_copy, by)

    def last_states():
        entering()
        states()

    def await_local():
        for seg in range(4):
            go(rows_copy, seg)
        for core in range(2):
            go(edge_copy, core, 1 - c)
        small_arrays()
        for copy in local[14:]:
            copy.wait()

    stages = {
        "norm_own": (await_local, lambda i: norm_unit(c, i), after_own),
        "norm_other": (before_other, lambda i: norm_unit(1 - c, i), None),
        "norm_edges": (before_edges, lambda i: norm_edges(), None),
        "source": (None, source, None),
        "source_edges": (None, lambda i: source_edges(), None),
        "spots": (None, lambda i: before_gates(), None),
        "gates": (None, gates, None),
        "gates_shake": (None, gates_shake, None),
        "totals": (None, lambda i: totals(), lambda: tell(0)),
        "hear0": (None, lambda i: hear(0), None),
        "hear1": (None, lambda i: hear(1), None),
        "hear2": (None, lambda i: hear(2), None),
        "shake_edges": (None, lambda i: shake_edges(), None),
        "exit_gate": (None, exit_gate, None),
        "conv": (None, conv, lambda: go(swap, 1)),
        "states": (None, lambda i: last_states(), lambda: go(swap, 0)),
        "result": (before_result, result, None),
    }
    held = {0: local[0:3], 1: local[3:5], 2: local[5:7], 3: out_local}
    units = {name: count for name, count, _, _ in STAGES}

    def follow(step):
        if step[0] == "send":
            for copy in held.pop(step[1][0], ()):
                copy.wait()
            go(message, step[1])
        elif step[0] == "wait":
            group_here(step[1])
        else:
            stages[step[1]][1](0)

    order, _ = plan()
    n = 0
    while n < len(order):
        step = order[n]
        if step[0] != "unit" or units[step[1]] == 1:
            if step[0] == "unit":
                before, work, after = stages[step[1]]
                with jax.named_scope(step[1]):
                    if before is not None:
                        before()
                    work(0)
                    if after is not None:
                        after()
            else:
                with jax.named_scope("_".join(str(v) for v in (step[0],) + step[1])):
                    follow(step)
            n += 1
            continue
        name = step[1]
        count = units[name]
        between = {}
        i = 0
        n += 1
        while i + 1 < count:
            if order[n] == ("unit", name, i + 1):
                i += 1
            else:
                between.setdefault(i, []).append(order[n])
            n += 1
        before, work, after = stages[name]
        with jax.named_scope(name):
            if before is not None:
                before()

            def one(k, _):
                with jax.named_scope("unit"):
                    work(k)
                for at, todo in between.items():

                    @pl.when(k == at)
                    def _():
                        for item in todo:
                            with jax.named_scope("_".join(str(v) for v in ((item[0],) + item[1] if item[0] != "unit" else item))):
                                follow(item)

                return 0

            lax.fori_loop(0, count, one, 0)
            if after is not None:
                after()
    for i in range(2):
        for seg in range(4):
            write(i, seg).wait()
    with jax.named_scope("drain"):
        for n in range(max(0, len(sends) - POOL), len(sends)):
            finish(n)


def body(
    activation_sequence,
    rms_multiplier_vector,
    linear_memory_source_matrix,
    linear_memory_exit_matrix,
    filter_exit_mask_matrix,
    filter_entry_mask_matrix,
    filter_source_matrix,
    memory_prefilter_taps,
    filter_taps_depthwise,
    fading_mask_diagonal_tiles,
    entry_mask_diagonal_tiles,
    fading_speed_per_channel,
    speed_multiplier,
    jump_per_position,
    boundary_hidden_vectors,
    final_mixing_matrix,
):
    dma = pltpu.SemaphoreType.DMA
    mixed = pl.pallas_call(
        kernel,
        name="layer",
        out_shape=jax.ShapeDtypeStruct((256, 2, WIDE), bf16),
        in_specs=[pl.BlockSpec(memory_space=pl.ANY)] * 16,
        out_specs=pl.BlockSpec(memory_space=pl.ANY),
        scratch_shapes=[
            pltpu.VMEM((2, STEPS, 4, 2, WIDE), bf16),
            pltpu.VMEM((4, 2, WIDE), bf16),
            pltpu.VMEM((2 * OWN + 32, WIDE), bf16),
            pltpu.VMEM((4, 4, 4, W_END, LANES), bf16),
            pltpu.VMEM((4, 4, 4, 2, OUT_ROWS, LANES), bf16),
            pltpu.VMEM((16, LANES), bf16),
            pltpu.VMEM((4, LANES), bf16),
            pltpu.VMEM((3, LANES), bf16),
            pltpu.VMEM((2, LANES), f32),
            pltpu.VMEM((2, 2, LANES), f32),
            pltpu.VMEM((2, 16, LANES), f32),
            pltpu.VMEM((4, 16, LANES), f32),
            pltpu.VMEM((2, 1024, LANES), f32),
            pltpu.VMEM((2, 2, 544, 256), f32),
            pltpu.VMEM((2, 2, 544, 256), f32),
            pltpu.VMEM((2, 32, 256), f32),
            pltpu.VMEM((2, 2, 2, OWN, 256), f32),
            pltpu.VMEM((2, 2, 2, OWN, 256), f32),
            pltpu.VMEM((2, 2, OWN, 256), f32),
            pltpu.VMEM((2, 2, 4, OWN, LANES), bf16),
            pltpu.VMEM((2, 4, OWN, LANES), bf16),
            pltpu.VMEM((2, 2, 2, 2, 8, 256), f32),
            pltpu.VMEM((3, 2, 2, 2, 8, 256), f32),
            pltpu.VMEM((3, 4, 8, 512), f32),
            pltpu.VMEM((STEPS, 4, 2, WIDE), bf16),
            dma((18,)),
            dma((16,)),
            dma((POOL,)),
            dma((first_place(len(PIECES) - 1, 3),)),
            dma((3,)),
            dma((4,)),
            dma((2,)),
            dma((3,)),
            dma((9,)),
            dma((2,)),
            dma((2, 4)),
        ],
        compiler_params=pltpu.CompilerParams(
            collective_id=0, has_side_effects=True, vmem_limit_bytes=54 * 1024 * 1024
        ),
    )(
        activation_sequence,
        rms_multiplier_vector.reshape(16, LANES),
        linear_memory_source_matrix,
        linear_memory_exit_matrix,
        filter_exit_mask_matrix,
        filter_entry_mask_matrix,
        filter_source_matrix,
        memory_prefilter_taps,
        filter_taps_depthwise,
        fading_mask_diagonal_tiles.reshape(256, LANES),
        entry_mask_diagonal_tiles.reshape(256, LANES),
        fading_speed_per_channel,
        speed_multiplier.reshape(16, LANES),
        jump_per_position.reshape(16, LANES),
        boundary_hidden_vectors,
        final_mixing_matrix.transpose(0, 2, 1),
    )
    return pl.pallas_call(
        hand_over,
        name="hand_over",
        out_shape=jax.ShapeDtypeStruct(mixed.shape, bf16),
        in_specs=[pl.BlockSpec(memory_space=pl.ANY)],
        out_specs=pl.BlockSpec(memory_space=pl.ANY),
        scratch_shapes=[pltpu.VMEM((256, 2, WIDE), bf16), dma((8,)), dma((8,))],
    )(mixed)


def hand_over(src, dst, held, in_sem, out_sem):
    parts = [pl.ds(n * 32, 32) for n in range(8)]
    reads = [pltpu.make_async_copy(src.at[p], held.at[p], in_sem.at[n]) for n, p in enumerate(parts)]
    writes = [pltpu.make_async_copy(held.at[p], dst.at[p], out_sem.at[n]) for n, p in enumerate(parts)]
    for copy in reads:
        copy.start()
    for a, b in zip(reads, writes):
        a.wait()
        b.start()
    for copy in writes:
        copy.wait()


def solution(mesh):
    return jax.shard_map(
        body,
        mesh=mesh,
        in_specs=(
            P(("sp", "tp"), None, None),
            P(),
            P("sp", "tp"),
            P("sp", "tp"),
            P("sp", "tp"),
            P("sp", "tp"),
            P("sp", "tp"),
            P(None, "tp"),
            P(None, "tp"),
            P(None, "tp", None, None),
            P(None, "tp", None, None),
            P(None, "tp"),
            P("sp"),
            P("sp"),
            P(None, None, "tp"),
            P(None, None, ("sp", "tp")),
        ),
        out_specs=P(("sp", "tp"), None, None),
        check_vma=False,
    )
```

```python
import jax
import jax.numpy as jnp
from jax import lax
from jax.experimental import pallas as pl
from jax.experimental.pallas import tpu as pltpu
from jax.sharding import PartitionSpec as P

MESH = pl.DeviceIdType.MESH
f32, bf16 = jnp.float32, jnp.bfloat16

EPS = 1e-06
RING = 4
OWN = 512
STEPS = 64
WIDE = 2048
LANES = 128
POOL = 48

SRC, GATES, CGATE, CIN, COUT, EXIT, W_END = 0, 128, 160, 288, 416, 544, 672
OUT_ROWS = 256

PIECES = (
    ("w", ((0, 64), (64, 112), (112, 160))),
    ("w", ((160, 240), (240, 320), (320, 416))),
    ("w", ((416, 496), (496, 592), (592, 672))),
    ("o", ((0, 80), (80, 160), (160, 256))),
)
FINE = (True, True, True, True)
FAR = ()
ORDERS = (("y", "x", "z"), ("x", "z", "y"), ("z", "y", "x"))
NEAR = (0, -1, 1, 2)
FORWARD = {1: (0, -1), -1: (1, 2)}


def turn_of(piece):
    return 1 if piece % 2 == 0 else -1


def places(piece):
    return 7 if FINE[piece] else 5


def first_place(piece, colour):
    return sum(3 * (3 + 2 * places(p)) for p in range(piece)) + colour * (3 + 2 * places(piece))


def group_of(m):
    piece, colour, phase, kind, way, r = m
    if kind == "pass":
        return (piece, colour, 3, 0, 4)
    if phase == 0:
        return (piece, colour, 0, 2 if kind != "own" else (0 if way == 1 else 1), 1)
    first = 3 + places(piece) * (phase - 1)
    if kind != "own":
        return (piece, colour, phase, first + places(piece) - 1, 4 if FINE[piece] else 2)
    if not FINE[piece]:
        return (piece, colour, phase, first + (r if way == 1 else 3 - r), 1)
    alone = FORWARD[way]
    place = alone.index(r) if r in alone else 2
    return (piece, colour, phase, first + place + (0 if way == 1 else 3), 1 if r in alone else 2)


def messages(piece, colour):
    found = {}
    up = turn_of(piece)
    fine = FINE[piece]

    def one(phase, kind, way, r):
        return (piece, colour, phase, kind, way, r)

    def here(*given):
        return tuple(dict.fromkeys(group_of(m) for m in given))

    def both(phase, r, needs):
        for way in (1, -1):
            found[one(phase, "own", way, r)] = needs

    both(0, 0, ())
    if (piece, 0) in FAR:
        opposite = one(0, "far", up, 0)
        found[opposite] = ()
    else:
        opposite = one(0, "fwd", up, 0)
        found[opposite] = here(one(0, "own", up, 0))
    near = [one(0, "own", 1, 0), one(0, "own", -1, 0)]
    before = here(*near, opposite)
    ready = {0: (), -1: here(near[0]), 1: here(near[1]), 2: here(opposite)}
    for phase in (1, 2):
        for r in NEAR if fine else (0, 1):
            both(phase, r, ready[r] if fine else before)
        last = []
        if (piece, phase) in FAR:
            for r in NEAR:
                last.append(one(phase, "far", up, r))
                found[last[-1]] = ready[r]
        else:
            for way in (1, -1):
                for r in FORWARD[way] if fine else ((0,) if way == 1 else (1,)):
                    last.append(one(phase, "fwd", way, r))
                    found[last[-1]] = here(one(phase, "own", way, r))
        parts = NEAR if fine else (0, 1)
        ready = {
            0: before,
            -1: here(*(one(phase, "own", 1, r) for r in parts)),
            1: here(*(one(phase, "own", -1, r) for r in parts)),
            2: here(*last),
        }
        if phase == 2:
            break
        before = before + ready[-1] + ready[1] + ready[2]
    if PIECES[piece][0] == "o":
        for slot, r in enumerate(NEAR):
            found[one(3, "pass", 0, slot)] = before if r == 0 else ready[r]
    return found


def size(m):
    first, last = PIECES[m[0]][1][m[1]]
    chunks = (1, 1, 4, 16)[m[2]] * (1 if FINE[m[0]] or m[2] in (0, 3) else 2)
    return (last - first) * 0.25 * chunks * (2 if m[3] == "far" else 1)


RATE, HOP = 47.0, 2.8
SIDE_RATE, SIDE_HOP = 450.0, 1.4

STAGES = (
    ("norm_own", 8, 0.79, ()),
    ("norm_other", 8, 0.79, ("rows",)),
    ("norm_edges", 1, 0.3, ("edges",)),
    ("spots", 1, 0.8, ("small",)),
    ("source", 4, 0.78, ("norm_own", "norm_other", "norm_edges", 0)),
    ("source_edges", 1, 0.6, ("source",)),
    ("gates", 2, 1.65, ("source_edges", "spots")),
    ("gates_shake", 4, 1.85, ("gates", 1)),
    ("totals", 1, 1.3, ("gates_shake",)),
    ("hear0", 1, 0.4, ("told0",)),
    ("hear1", 1, 0.4, ("told1",)),
    ("hear2", 1, 0.5, ("told2",)),
    ("shake_edges", 1, 0.8, ("gates_shake",)),
    ("exit_gate", 2, 1.5, (2, "norm_other")),
    ("conv", 2, 1.5, (2, "shake_edges")),
    ("states", 1, 1.5, ("hear2", "exit_gate")),
    ("result", 4, 1.5, (3, "swapped0", "swapped1")),
)
BACKLOG = 1.5


def PRIORITY(m):
    return (m[0], m[2])


def plan():
    deps = {}
    for piece in range(len(PIECES)):
        for colour in range(3):
            deps.update(messages(piece, colour))
    groups = {}
    for m in deps:
        groups.setdefault(group_of(m), []).append(m)
    clock, link, coming, arrive, sent, got = 0.0, {}, {}, {}, set(), set()
    times = {"rows": 6.0, "edges": 4.0, "small": 6.0}
    order, done, progress = [], set(), {}

    def send_ready():
        ready = [m for m in deps if m not in sent and all(d in got for d in deps[m])]
        for m in sorted(ready, key=PRIORITY):
            side = m[3] == "pass"
            wire = "side" if side else (ORDERS[m[1]][m[2]], m[4])
            if link.get(wire, 0.0) - clock > BACKLOG:
                continue
            link[wire] = max(clock, link.get(wire, 0.0)) + size(m) / (SIDE_RATE if side else RATE)
            arrive[m] = link[wire] + (SIDE_HOP if side else HOP + (0.8 if m[3] == "far" else 0.0))
            sent.add(m)
            order.append(("send", m))
            g = group_of(m)
            if all(n in sent for n in groups[g]):
                coming[g] = max(arrive[n] for n in groups[g])

    def met(need):
        if isinstance(need, int):
            return all(g in got for g in groups if g[0] == need)
        return need in done or times.get(need, 1e9) <= clock

    current = None
    send_ready()
    while len(done) < len(STAGES):
        here = sorted((m for m in coming if m not in got and coming[m] <= clock), key=lambda m: (m[0], coming[m]))
        if here:
            m = here[0]
            got.add(m)
            order.append(("wait", m))
            clock += 0.03
            send_ready()
            continue
        send_ready()
        if current is None:
            for n, stage in enumerate(STAGES):
                if stage[0] not in done and all(met(need) for need in stage[3]):
                    current = stage
                    break
        quick = next(
            (st for st in STAGES if st[0].startswith("hear") and st[0] not in done and all(met(k) for k in st[3])), None
        )
        if quick is not None:
            order.append(("unit", quick[0], 0))
            clock += quick[2]
            done.add(quick[0])
            level = int(quick[0][4])
            if level < 2:
                times[f"told{level + 1}"] = clock + 3.5
            if current is quick:
                current = None
            continue
        if current is not None:
            name, units, cost, _ = current
            i = progress.get(name, 0)
            order.append(("unit", name, i))
            clock += cost
            progress[name] = i + 1
            if i + 1 == units:
                done.add(name)
                current = None
                if name == "totals":
                    times["told0"] = clock + 3.5
                if name == "conv":
                    times["swapped1"] = clock + 3.0
                if name == "states":
                    times["swapped0"] = clock + 3.0
            continue
        if any(m not in sent and all(d in got for d in deps[m]) for m in deps):
            clock += 0.25
            continue
        later = [t for m, t in coming.items() if m not in got] + [t for t in times.values() if t > clock]
        clock = min(t for t in later if t > clock)
    return order, clock


def wrap(i):
    return lax.rem(i + RING, RING)


def rows_of(shape):
    return lax.broadcasted_iota(jnp.int32, shape, 0)


def turn(v, by):
    return pltpu.roll(v, by, 0)


def spread(v, first):
    row = rows_of(v.shape)
    v = jnp.where((row >= first) & (row < first + 2), v, 0.0)
    v = v + turn(v, 2)
    return v + turn(v, 4)


def kernel(
    x_in, gain_in, src_in, exit_in, cout_in, cgate_in, cin_in, taps_in, ctaps_in, fade_in, entry_in, speed_in,
    tempo_in, jump_in, edge_in, out_w, out,
    XR, XE, X, G, Wo, GN, TB, CB, SB, BB, PM, SM, MJ, Rp, Sp, Hh, A, U, GL, ACT, ACTS, SEG, PRE, XS, OUT,
    lsem, wsem, pool, grecv, frecv, xrecv, hrecv, srecv, erecv, arecv, osem,
):
    sp, tp = lax.axis_index("sp"), lax.axis_index("tp")
    me = {"z": sp // 4, "x": lax.rem(sp, 4), "y": tp // 2}
    c = lax.rem(tp, 2)
    z, x, y = me["z"], me["x"], me["y"]
    q = sp * 4 + y

    def device(at, core):
        return {"sp": at["z"] * 4 + at["x"], "tp": at["y"] * 2 + core}

    def along(d, by):
        return {**me, d: wrap(me[d] + by)}

    sibling = device(me, 1 - c)
    ahead = lax.rem(q + 1, 64)
    behind = lax.rem(q + 63, 64)

    def chip(number, core):
        return {"sp": number // 4, "tp": lax.rem(number, 4) * 2 + core}

    barrier = pltpu.get_barrier_semaphore()

    def hello(to):
        pl.semaphore_signal(barrier, inc=1, device_id=to, device_id_type=MESH)

    hello(sibling)
    for d in ("z", "x", "y"):
        for by in (1, 2, 3):
            hello(device(along(d, by), c))
    hello(chip(behind, 1))
    hello(chip(ahead, 0))

    def own_rows(first, count):
        return G.at[z, x, y, pl.ds(first, count)]

    sp16 = pl.ds(pl.multiple_of(sp * 16, 16), 16)
    pairs = [
        (src_in, own_rows(SRC, 128)),
        (fade_in.at[sp16], own_rows(GATES, 16)),
        (entry_in.at[sp16], own_rows(GATES + 16, 16)),
        (cgate_in, own_rows(CGATE, 128)),
        (cin_in, own_rows(CIN, 128)),
        (cout_in, own_rows(COUT, 128)),
        (exit_in, own_rows(EXIT, 128)),
        (gain_in, GN),
        (taps_in, TB),
        (ctaps_in, CB),
        (speed_in, SB),
        (edge_in, BB),
        (tempo_in, PM.at[0]),
        (jump_in, PM.at[1]),
    ]
    pairs += [(x_in.at[pl.ds(seg * STEPS, STEPS)], XR.at[c, :, seg]) for seg in range(4)]
    local = [pltpu.make_async_copy(a, b, lsem.at[n]) for n, (a, b) in enumerate(pairs)]
    out_local = [
        pltpu.make_async_copy(
            out_w.at[n // 8, :, pl.ds((n % 8) * LANES, LANES)], Wo.at[z, x, y, c, pl.ds(n * 16, 16)], wsem.at[n]
        )
        for n in range(16)
    ]
    for copy in local + out_local:
        copy.start()
    pl.semaphore_wait(barrier, 12)

    def remote(src, dst, send, recv, to):
        return pltpu.make_async_remote_copy(
            src_ref=src, dst_ref=dst, send_sem=pool.at[0] if send is None else send, recv_sem=recv, device_id=to, device_id_type=MESH
        )

    sends = []

    def go(make, *given):
        n = len(sends)
        if n >= POOL:
            finish(n - POOL)
        make(*given, send=pool.at[n % POOL]).start()
        sends.append((make, given))

    def finish(n):
        make, given = sends[n]
        make(*given, send=pool.at[n % POOL]).wait_send()

    def rows_copy(seg, send=None):
        return remote(
            x_in.at[pl.ds(seg * STEPS, STEPS)], XR.at[c, :, seg], send, xrecv.at[seg], sibling
        )

    target = jnp.where(c == 1, ahead, behind)

    def edge_copy(core, slot, send=None):
        return remote(
            x_in.at[pl.ds(c * 254, 2)], XE.at[pl.ds((1 - c) * 2, 2)], send, hrecv.at[slot], chip(target, core)
        )

    def region(piece, colour, phase, i, r, count=1):
        kind, parts = PIECES[piece]
        first, last = parts[colour]
        a, b, d = ORDERS[colour]
        where = dict(me)
        if phase == 0:
            where[a] = i
        elif phase < 3:
            cut = (a, b)[phase - 1]
            if phase == 2:
                where[a] = slice(None)
            where[(b, d)[phase - 1]] = i
            if FINE[piece]:
                where[cut] = wrap(me[cut] + r) if count == 1 else pl.ds(0, count)
            else:
                where[cut] = pl.ds(2 * r, 2) if count == 1 else slice(None)
        else:
            where[a], where[b] = slice(None), slice(None)
            where[d] = i if count == 1 else slice(None)
        rows = pl.ds(first, last - first)
        if kind == "w":
            return G.at[where["z"], where["x"], where["y"], rows]
        return Wo.at[where["z"], where["x"], where["y"], c, rows]

    def message(m, send=None):
        piece, colour, phase, kind, way, r = m
        if kind == "pass":
            d = ORDERS[colour][2]
            ref = region(piece, colour, 3, wrap(me[d] + NEAR[r]), 0)
            return remote(ref, ref, send, frecv.at[(piece - 3) * 3 + colour], sibling)
        d = ORDERS[colour][phase]
        block = wrap(me[d] - way) if kind == "fwd" else me[d]
        ref = region(piece, colour, phase, block, r)
        at = first_place(piece, colour) + group_of(m)[3]
        return remote(ref, ref, send, grecv.at[at], device(along(d, 2 if kind == "far" else way), c))

    def group_here(g):
        piece, colour, phase, place, count = g
        ref = region(piece, colour, phase, 0, 0, count)
        at = frecv.at[(piece - 3) * 3 + colour] if phase == 3 else grecv.at[first_place(piece, colour) + place]
        remote(ref, ref, None, at, sibling).wait_recv()

    def small_arrays():
        for copy in local[7:14]:
            copy.wait()
        for row in range(4):
            SM[y, row : row + 1, :] = TB[row : row + 1, :].astype(f32)
        for row in range(3):
            SM[y, 4 + row : 5 + row, :] = CB[row : row + 1, :].astype(f32)
        for row in range(2):
            SM[y, 7 + row : 8 + row, :] = SB[row : row + 1, :]
            for b in range(2):
                SM[y, 9 + 2 * row + b : 10 + 2 * row + b, :] = BB[row, b : b + 1, :]
        SM[y, 13:16, :] = jnp.zeros((3, LANES), f32)

    def small_copy(by, send=None):
        return remote(SM.at[y], SM.at[y], send, srecv.at[by - 1], device(along("y", by), c))

    def positions():
        seg = rows_of((8, LANES)) // 2
        for n in range(2):
            for rc in range(2):
                lines = [
                    jnp.broadcast_to(PM[n, pl.ds(4 * y + rc * 2 + k, 1), :], (8, LANES)) for k in range(2)
                ]
                v = jnp.where(
                    seg == 0,
                    lines[0],
                    jnp.where(
                        seg == 1, pltpu.roll(lines[0], 64, 1), jnp.where(seg == 2, lines[1], pltpu.roll(lines[1], 64, 1))
                    ),
                )
                for j in range(STEPS):
                    MJ[n, rc * OWN + j * 8 : rc * OWN + j * 8 + 8, :] = jnp.broadcast_to(v[:, j : j + 1], (8, LANES))

    def scaled(parts, alive=None):
        total = parts[0] * parts[0]
        for v in parts[1:]:
            total = total + v * v
        r = lax.rsqrt(jnp.sum(total, axis=1, keepdims=True) * (1.0 / WIDE) + EPS)
        if alive is not None:
            r = r * alive
        r = jnp.broadcast_to(r, parts[0].shape)
        return [(v * r) * GN[n : n + 1, :].astype(f32) for n, v in enumerate(parts)]

    def norm_unit(rc, i):
        def one(k, _):
            j = i * 8 + k * 2
            parts = [
                XR[rc, pl.ds(j, 2), :, :, n * LANES : (n + 1) * LANES].astype(f32).reshape(16, LANES) for n in range(16)
            ]
            rows = pl.ds(pl.multiple_of(rc * OWN + j * 8, 16), 16)
            for n, v in enumerate(scaled(parts)):
                X[rows, n * LANES : (n + 1) * LANES] = v.astype(bf16)
            return 0

        lax.fori_loop(0, 4, one, 0)

    def norm_edges():
        row = rows_of((8, 1))
        alive = jnp.where(row < 4, jnp.where(q > 0, 1.0, 0.0), jnp.where(q < 63, 1.0, 0.0))
        parts = [XE[:, :, n * LANES : (n + 1) * LANES].astype(f32).reshape(8, LANES) for n in range(16)]
        for n, v in enumerate(scaled(parts, alive)):
            lane = slice(n * LANES, (n + 1) * LANES)
            X[2 * OWN : 2 * OWN + 16, lane] = jnp.concatenate([turn(v, 6), turn(v, 4)], axis=0).astype(bf16)
            X[2 * OWN + 16 : 2 * OWN + 32, lane] = jnp.concatenate([turn(v, 4), turn(v, 4)], axis=0).astype(bf16)

    def weight(row, yp):
        parts = [G[:, :, 2 * yp + h, pl.ds(row, LANES), :].reshape(WIDE, LANES) for h in range(2)]
        return jnp.concatenate(parts, axis=1)

    def project(rows, w):
        return jnp.dot(X[rows, :], w, preferred_element_type=f32)

    def wide(work, i):
        w = jnp.concatenate([G[:, :, y4, pl.ds(work[0], LANES), :].reshape(WIDE, LANES) for y4 in range(4)], axis=1)
        v = project(pl.ds(pl.multiple_of(i * OWN, OWN), OWN), w)
        for yp in range(2):
            work[1](yp, i, v[:, yp * 256 : (yp + 1) * 256])

    def block(work, i):
        yp, rc = i // 2, lax.rem(i, 2)
        work(yp, rc, pl.ds(pl.multiple_of(rc * OWN, OWN), OWN))

    main = pl.ds(16, OWN)
    edges = pl.ds(2 * OWN, 32)

    def pads(Rp):
        for yp in range(2):
            row = rows_of((8, 256))
            for rc in range(2):
                for j in range(2):
                    own = Rp[yp, rc, pl.ds(16 + (STEPS - 2 + j) * 8, 8), :]
                    prior = Hh[yp, pl.ds(8 * j, 8), :] if rc == 0 else Rp[yp, 0, pl.ds(16 + (STEPS - 2 + j) * 8, 8), :]
                    Rp[yp, rc, pl.ds(8 * j, 8), :] = jnp.where(row < 2, turn(prior, 2), turn(own, 2))
                own = Rp[yp, rc, pl.ds(16, 8), :]
                later = Rp[yp, 1, pl.ds(16, 8), :] if rc == 0 else Hh[yp, pl.ds(16, 8), :]
                Rp[yp, rc, pl.ds(16 + OWN, 8), :] = jnp.where(row >= 6, turn(later, 6), turn(own, 6))

    def source(i):
        def work(yp, rc, rows):
            Rp[yp, rc, main, :] = project(rows, weight(SRC, yp))

        block(work, i)

    def source_edges():
        for yp in range(2):
            Hh[yp] = project(edges, weight(SRC, yp))
        pads(Rp)

    def taps(yp, row):
        return jnp.concatenate([SM[2 * yp + h, pl.ds(row, 1), :] for h in range(2)], axis=1)

    GB = 128

    def gates(i):
        def one(k, _):
            gate_rows(0, i, k)
            return 0

        lax.fori_loop(0, 4, one, 0)

    def gate_rows(yp, rc, blk):
        base = pl.multiple_of(blk * GB, GB)
        rc_rows = taps(yp, 0) * Rp[yp, rc, pl.ds(base, GB), :]
        for k in range(1, 4):
            rc_rows = rc_rows + taps(yp, k) * Rp[yp, rc, pl.ds(base + 8 * k, GB), :]
        narrow = (0.5 * rc_rows).astype(bf16)
        half = narrow.astype(f32)
        at = pl.ds(pl.multiple_of(rc * OWN + blk * GB, GB), GB)
        tempo, jump = MJ[0, at, :], MJ[1, at, :]
        for h in range(2):
            lane = slice(h * LANES, (h + 1) * LANES)
            yy = 2 * yp + h
            maps = [
                G[pl.ds(2 * d, 2), :, yy, pl.ds(GATES + 16 * kind, 16), :].reshape(LANES, LANES)
                for kind in range(2)
                for d in range(2)
            ]
            for d in range(2):
                pre = jnp.dot(
                    narrow[:, lane], jnp.concatenate([maps[d], maps[2 + d]], axis=1), preferred_element_type=f32
                )
                speed = SM[yy, pl.ds(7 + d, 1), :] * -4.0
                la = (1.0 + jnp.tanh(pre[:, :LANES])) * (speed * tempo) + jump
                decay = jnp.exp(la)
                near = la * (-2.0 - la * (2.0 + la * (4.0 / 3.0)))
                rest = jnp.where(la > -0.005, near, 1.0 - decay * decay)
                root = rest * lax.rsqrt(jnp.maximum(rest, 1e-36))
                A[d, yp, rc, pl.ds(base, GB), lane] = decay
                U[d, yp, rc, pl.ds(base, GB), lane] = root * (1.0 + jnp.tanh(pre[:, LANES:])) * half[:, lane]

    PAIRS = [(yp, rc) for yp in range(2) for rc in range(2)]

    def tile(ref, d, yp, rc, j):
        return ref[d, yp, rc, pl.ds(pl.multiple_of(j * 8, 8), 8), :]

    def totals():
        def one(i, state):
            new = []
            for d in range(2):
                j = i if d == 0 else STEPS - 1 - i
                for n, (yp, rc) in enumerate(PAIRS):
                    sa, sb = state[d * 4 + n]
                    a = tile(A, d, yp, rc, j)
                    new.append((sa * a, sb * a + tile(U, d, yp, rc, j)))
            return tuple(new)

        start = tuple((jnp.ones((8, 256), f32), jnp.zeros((8, 256), f32)) for _ in range(8))
        end = lax.fori_loop(0, STEPS, one, start)
        row = rows_of((8, 256))
        for yp in range(2):
            whole = []
            for d in range(2):
                ends = []
                for rc in range(2):
                    a, b = end[d * 4 + yp * 2 + rc]
                    for by in (2, 4):
                        shift = by if d == 0 else 8 - by
                        inside = (row >= by) if d == 0 else (row < 8 - by)
                        pa, pb = turn(a, shift), turn(b, shift)
                        b = jnp.where(inside, a * pb + b, b)
                        a = jnp.where(inside, a * pa, a)
                    SEG[d, yp, rc, 0], SEG[d, yp, rc, 1] = a, b
                    ends.append((spread(a, 6 if d == 0 else 0), spread(b, 6 if d == 0 else 0)))
                first, second = ends if d == 0 else ends[::-1]
                whole.append((first[0] * second[0], second[0] * first[1] + second[1]))
            put(0, y, yp, whole)

    def put(level, slot, yp, whole):
        row = rows_of((8, 256))
        (fa, fb), (ba, bb) = whole
        XS[level, slot, :, yp * 256 : (yp + 1) * 256] = jnp.where(
            row < 2, fa, jnp.where(row < 4, fb, jnp.where(row < 6, ba, bb))
        )

    AXES = ("y", "x", "z")

    def share(level, by, send=None):
        d = AXES[level]
        ref = XS.at[level, me[d]]
        k = level * 3 + by - 1
        return remote(ref, ref, send, erecv.at[k], device(along(d, by), c))

    def tell(level):
        for by in (1, 2, 3):
            go(share, level, by)

    def combine(early, late):
        return early[0] * late[0], late[0] * early[1] + late[1]

    def hear(level):
        for by in (1, 2, 3):
            share(level, by).wait_recv()
        m = me[AXES[level]]
        for yp in range(2):
            one = (jnp.ones((8, 256), f32), jnp.zeros((8, 256), f32))
            whole = []
            for d in range(2):
                total, prefix = one, one
                for i in range(4) if d == 0 else range(3, -1, -1):
                    v = XS[level, i, :, yp * 256 : (yp + 1) * 256]
                    item = (spread(v, 4 * d), spread(v, 4 * d + 2))
                    passed = (i < m) if d == 0 else (i > m)
                    longer = combine(prefix, item)
                    prefix = tuple(jnp.where(passed, n, o) for n, o in zip(longer, prefix))
                    total = combine(total, item)
                whole.append(total)
                PRE[level, yp, d, 0], PRE[level, yp, d, 1] = prefix
            if level < 2:
                put(level + 1, me[AXES[level + 1]], yp, whole)
        if level < 2:
            tell(level + 1)

    def entering():
        row = rows_of((8, 256))
        even = (row % 2) == 0
        for yp in range(2):
            for d in range(2):
                h = jnp.where(even, taps(yp, 9 + 2 * d), taps(yp, 10 + 2 * d))
                for level in (2, 1, 0):
                    a, b = PRE[level, yp, d, 0], PRE[level, yp, d, 1]
                    h = a * h + b
                for rc in (0, 1) if d == 0 else (1, 0):
                    a, b = SEG[d, yp, rc, 0], SEG[d, yp, rc, 1]
                    shift = 2 if d == 0 else 6
                    inside = (row >= 2) if d == 0 else (row < 6)
                    pa = jnp.where(inside, turn(a, shift), 1.0)
                    pb = jnp.where(inside, turn(b, shift), 0.0)
                    SEG[d, yp, rc, 0] = pa * h + pb
                    last = 6 if d == 0 else 0
                    h = spread(a, last) * h + spread(b, last)

    def exit_gate(i):
        def work(yp, rc, v):
            inner = v * (0.7978845608028654 + 0.035677408136300125 * v * v)
            GL[yp, rc] = 0.5 * v * (1.0 + jnp.tanh(inner))

        wide((EXIT, work), i)

    def states():
        def forth(i, state):
            new = []
            for n, (yp, rc) in enumerate(PAIRS):
                h = tile(A, 0, yp, rc, i) * state[n] + tile(U, 0, yp, rc, i)
                U[0, yp, rc, pl.ds(pl.multiple_of(i * 8, 8), 8), :] = h
                new.append(h)
            return tuple(new)

        def back(i, state):
            new = []
            low = STEPS - 2 - 2 * i
            rows16 = pl.ds(pl.multiple_of(low * 8, 16), 16)
            for n, (yp, rc) in enumerate(PAIRS):
                h1 = tile(A, 1, yp, rc, low + 1) * state[n] + tile(U, 1, yp, rc, low + 1)
                h0 = tile(A, 1, yp, rc, low) * h1 + tile(U, 1, yp, rc, low)
                both = jnp.concatenate([h0, h1], axis=0) + U[0, yp, rc, rows16, :]
                done = (both * GL[yp, rc, rows16, :]).astype(bf16)
                for h in range(2):
                    ACT[rc, 0, 2 * yp + h, rows16, :] = done[:, h * LANES : (h + 1) * LANES]
                new.append(h0)
            return tuple(new)

        lax.fori_loop(0, STEPS, forth, tuple(SEG[0, yp, rc, 0] for yp, rc in PAIRS))
        lax.fori_loop(0, STEPS // 2, back, tuple(SEG[1, yp, rc, 0] for yp, rc in PAIRS))

    def shake(i):
        def work(yp, rc, rows):
            Sp[yp, rc, main, :] = project(rows, weight(CGATE, yp)) * project(rows, weight(CIN, yp))

        block(work, i)

    def gates_shake(i):
        shake(i)
        for k in range(2):
            gate_rows(1, i // 2, lax.rem(i, 2) * 2 + k)

    def shake_edges():
        for yp in range(2):
            Hh[yp] = project(edges, weight(CGATE, yp)) * project(edges, weight(CIN, yp))
        pads(Sp)

    def conv(i):
        def work(yp, rc, v):
            s = jnp.zeros((OWN, 256), f32)
            for k in range(3):
                s = s + taps(yp, 4 + k) * Sp[yp, rc, pl.ds(8 + 8 * k, OWN), :]
            done = (v * s).astype(bf16)
            for h in range(2):
                ACT[rc, 1, 2 * yp + h] = done[:, h * LANES : (h + 1) * LANES]

        wide((COUT, work), i)

    def swap(m, send=None):
        return remote(ACT.at[1 - c, m], ACTS.at[m], send, arecv.at[m], sibling)

    def result(i):
        zz = i
        left, right = [], []
        for own in range(2):
            core = c if own == 0 else 1 - c
            for m in range(2):
                for yy in range(4):
                    left.append(ACT[c, m, yy] if own == 0 else ACTS[m, yy])
                    k16 = pl.ds(pl.multiple_of((m * 8 + 2 * yy + core) * 16, 16), 16)
                    right.append(Wo[zz, :, :, :, k16, :].reshape(512, LANES))
        v = lax.dot_general(
            jnp.concatenate(left, axis=1), jnp.concatenate(right, axis=1),
            (((1,), (1,)), ((), ())), preferred_element_type=f32,
        )
        OUT[:, :, :, pl.ds(pl.multiple_of(i * 512, 512), 512)] = v.astype(bf16).reshape(STEPS, 4, 2, 512)

        @pl.when(lax.rem(i, 2) == 1)
        def _():
            for seg in range(4):
                write(i // 2, seg).start()

    def write(i, seg):
        lanes = pl.ds(pl.multiple_of(i * 1024, 1024), 1024)
        return pltpu.make_async_copy(OUT.at[:, seg, :, lanes], out.at[pl.ds(seg * STEPS, STEPS), :, lanes], osem.at[i, seg])

    def before_other():
        for seg in range(4):
            rows_copy(seg).wait_recv()

    def before_edges():
        for slot in range(2):
            edge_copy(0, slot).wait_recv()

    def before_gates():
        for by in (1, 2, 3):
            small_copy(by).wait_recv()
        positions()

    def before_result():
        for m in (1, 0):
            swap(m).wait_recv()

    def after_own():
        for by in (1, 2, 3):
            go(small_copy, by)

    def last_states():
        entering()
        states()

    def await_local():
        for seg in range(4):
            go(rows_copy, seg)
        for core in range(2):
            go(edge_copy, core, 1 - c)
        small_arrays()
        for copy in local[14:]:
            copy.wait()

    stages = {
        "norm_own": (await_local, lambda i: norm_unit(c, i), after_own),
        "norm_other": (before_other, lambda i: norm_unit(1 - c, i), None),
        "norm_edges": (before_edges, lambda i: norm_edges(), None),
        "source": (None, source, None),
        "source_edges": (None, lambda i: source_edges(), None),
        "spots": (None, lambda i: before_gates(), None),
        "gates": (None, gates, None),
        "gates_shake": (None, gates_shake, None),
        "totals": (None, lambda i: totals(), lambda: tell(0)),
        "hear0": (None, lambda i: hear(0), None),
        "hear1": (None, lambda i: hear(1), None),
        "hear2": (None, lambda i: hear(2), None),
        "shake_edges": (None, lambda i: shake_edges(), None),
        "exit_gate": (None, exit_gate, None),
        "conv": (None, conv, lambda: go(swap, 1)),
        "states": (None, lambda i: last_states(), lambda: go(swap, 0)),
        "result": (before_result, result, None),
    }
    held = {0: local[0:3], 1: local[3:5], 2: local[5:7], 3: out_local}
    units = {name: count for name, count, _, _ in STAGES}

    def follow(step):
        if step[0] == "send":
            for copy in held.pop(step[1][0], ()):
                copy.wait()
            go(message, step[1])
        elif step[0] == "wait":
            group_here(step[1])
        else:
            stages[step[1]][1](0)

    order, _ = plan()
    n = 0
    while n < len(order):
        step = order[n]
        if step[0] != "unit" or units[step[1]] == 1:
            if step[0] == "unit":
                before, work, after = stages[step[1]]
                with jax.named_scope(step[1]):
                    if before is not None:
                        before()
                    work(0)
                    if after is not None:
                        after()
            else:
                with jax.named_scope("_".join(str(v) for v in (step[0],) + step[1])):
                    follow(step)
            n += 1
            continue
        name = step[1]
        count = units[name]
        between = {}
        i = 0
        n += 1
        while i + 1 < count:
            if order[n] == ("unit", name, i + 1):
                i += 1
            else:
                between.setdefault(i, []).append(order[n])
            n += 1
        before, work, after = stages[name]
        with jax.named_scope(name):
            if before is not None:
                before()

            def one(k, _):
                with jax.named_scope("unit"):
                    work(k)
                for at, todo in between.items():

                    @pl.when(k == at)
                    def _():
                        for item in todo:
                            with jax.named_scope("_".join(str(v) for v in ((item[0],) + item[1] if item[0] != "unit" else item))):
                                follow(item)

                return 0

            lax.fori_loop(0, count, one, 0)
            if after is not None:
                after()
    for i in range(2):
        for seg in range(4):
            write(i, seg).wait()
    with jax.named_scope("drain"):
        for n in range(max(0, len(sends) - POOL), len(sends)):
            finish(n)


def body(
    activation_sequence,
    rms_multiplier_vector,
    linear_memory_source_matrix,
    linear_memory_exit_matrix,
    filter_exit_mask_matrix,
    filter_entry_mask_matrix,
    filter_source_matrix,
    memory_prefilter_taps,
    filter_taps_depthwise,
    fading_mask_diagonal_tiles,
    entry_mask_diagonal_tiles,
    fading_speed_per_channel,
    speed_multiplier,
    jump_per_position,
    boundary_hidden_vectors,
    final_mixing_matrix,
):
    dma = pltpu.SemaphoreType.DMA
    mixed = pl.pallas_call(
        kernel,
        name="layer",
        out_shape=jax.ShapeDtypeStruct((256, 2, WIDE), bf16),
        in_specs=[pl.BlockSpec(memory_space=pl.ANY)] * 16,
        out_specs=pl.BlockSpec(memory_space=pl.ANY),
        scratch_shapes=[
            pltpu.VMEM((2, STEPS, 4, 2, WIDE), bf16),
            pltpu.VMEM((4, 2, WIDE), bf16),
            pltpu.VMEM((2 * OWN + 32, WIDE), bf16),
            pltpu.VMEM((4, 4, 4, W_END, LANES), bf16),
            pltpu.VMEM((4, 4, 4, 2, OUT_ROWS, LANES), bf16),
            pltpu.VMEM((16, LANES), bf16),
            pltpu.VMEM((4, LANES), bf16),
            pltpu.VMEM((3, LANES), bf16),
            pltpu.VMEM((2, LANES), f32),
            pltpu.VMEM((2, 2, LANES), f32),
            pltpu.VMEM((2, 16, LANES), f32),
            pltpu.VMEM((4, 16, LANES), f32),
            pltpu.VMEM((2, 1024, LANES), f32),
            pltpu.VMEM((2, 2, 544, 256), f32),
            pltpu.VMEM((2, 2, 544, 256), f32),
            pltpu.VMEM((2, 32, 256), f32),
            pltpu.VMEM((2, 2, 2, OWN, 256), f32),
            pltpu.VMEM((2, 2, 2, OWN, 256), f32),
            pltpu.VMEM((2, 2, OWN, 256), f32),
            pltpu.VMEM((2, 2, 4, OWN, LANES), bf16),
            pltpu.VMEM((2, 4, OWN, LANES), bf16),
            pltpu.VMEM((2, 2, 2, 2, 8, 256), f32),
            pltpu.VMEM((3, 2, 2, 2, 8, 256), f32),
            pltpu.VMEM((3, 4, 8, 512), f32),
            pltpu.VMEM((STEPS, 4, 2, WIDE), bf16),
            dma((18,)),
            dma((16,)),
            dma((POOL,)),
            dma((first_place(len(PIECES) - 1, 3),)),
            dma((3,)),
            dma((4,)),
            dma((2,)),
            dma((3,)),
            dma((9,)),
            dma((2,)),
            dma((2, 4)),
        ],
        compiler_params=pltpu.CompilerParams(
            collective_id=0, has_side_effects=True, vmem_limit_bytes=54 * 1024 * 1024
        ),
    )(
        activation_sequence,
        rms_multiplier_vector.reshape(16, LANES),
        linear_memory_source_matrix,
        linear_memory_exit_matrix,
        filter_exit_mask_matrix,
        filter_entry_mask_matrix,
        filter_source_matrix,
        memory_prefilter_taps,
        filter_taps_depthwise,
        fading_mask_diagonal_tiles.reshape(256, LANES),
        entry_mask_diagonal_tiles.reshape(256, LANES),
        fading_speed_per_channel,
        speed_multiplier.reshape(16, LANES),
        jump_per_position.reshape(16, LANES),
        boundary_hidden_vectors,
        final_mixing_matrix.transpose(0, 2, 1),
    )
    return pl.pallas_call(
        hand_over,
        name="hand_over",
        out_shape=jax.ShapeDtypeStruct(mixed.shape, bf16),
        in_specs=[pl.BlockSpec(memory_space=pl.ANY)],
        out_specs=pl.BlockSpec(memory_space=pl.ANY),
        scratch_shapes=[pltpu.VMEM((256, 2, WIDE), bf16), dma((8,)), dma((8,))],
    )(mixed)


def hand_over(src, dst, held, in_sem, out_sem):
    parts = [pl.ds(n * 32, 32) for n in range(8)]
    reads = [pltpu.make_async_copy(src.at[p], held.at[p], in_sem.at[n]) for n, p in enumerate(parts)]
    writes = [pltpu.make_async_copy(held.at[p], dst.at[p], out_sem.at[n]) for n, p in enumerate(parts)]
    for copy in reads:
        copy.start()
    for a, b in zip(reads, writes):
        a.wait()
        b.start()
    for copy in writes:
        copy.wait()


def solution(mesh):
    return jax.shard_map(
        body,
        mesh=mesh,
        in_specs=(
            P(("sp", "tp"), None, None),
            P(),
            P("sp", "tp"),
            P("sp", "tp"),
            P("sp", "tp"),
            P("sp", "tp"),
            P("sp", "tp"),
            P(None, "tp"),
            P(None, "tp"),
            P(None, "tp", None, None),
            P(None, "tp", None, None),
            P(None, "tp"),
            P("sp"),
            P("sp"),
            P(None, None, "tp"),
            P(None, None, ("sp", "tp")),
        ),
        out_specs=P(("sp", "tp"), None, None),
        check_vma=False,
    )
```
